32 devices in a mesh: sp: 4 (over y, x), tp: 8 (over z, core).
Axes of the slice: x: 2, y: 2, z: 4, core: 2. Of those that a mesh axis runs over, the one named last changes fastest.
Arguments:
- tokens: bfloat16 [2048, 4096], P('sp', 'tp'), may hold values from -6 to 6
- pre_gain: float32 [2, 4096], replicated, may hold values from 0.1 to 1.9
- w_value: bfloat16 [2, 4096, 4096], P(None, 'sp', 'tp'), may hold values from -0.09375 to 0.09375
- w_gate: bfloat16 [2, 4096, 4096], P(None, 'sp', 'tp'), may hold values from -0.09375 to 0.09375
- conv_taps: float32 [2, 31, 4096], P(None, None, 'tp'), may hold values from -3.5 to 3.5
- conv_bias: float32 [2, 4096], P(None, 'tp'), may hold values from -3 to 3
- norm_gain: float32 [2, 4096], P(None, 'tp'), may hold values from 0.1 to 1.9
- norm_bias: float32 [2, 4096], P(None, 'tp'), may hold values from -3 to 3
- w_out: bfloat16 [2, 4096, 4096], P(None, 'sp', 'tp'), may hold values from -0.09375 to 0.09375
- post_gain: float32 [2, 4096], P(None, 'tp'), may hold values from 0.1 to 1.9
Outputs:
- stream: bfloat16 [2048, 4096], P('sp', 'tp')
The draws below stay inside these ranges and needn't reach their ends.
All inputs are finite; a program needn't handle non-finite values.
Results may differ from the reference program's by a relative error of at most 0.009.
Values may be sent and summed in bfloat16 or wider, within the bound.
A program may use at most 64 MiB of HBM per device.

```python
import math
import jax
import jax.numpy as jnp
from jax import lax

D = 4096
CH = 4096
TAPS = 31
LAYERS = 2
TOKENS = 2048


def draw_conv_taps(key, part):
    first_key, second_key, third_key = jax.random.split(key, 3)
    channel = jnp.arange(CH, dtype=jnp.float32)
    phase = jax.random.uniform(first_key, (LAYERS, 1, 1), jnp.float32, 0.0, 2.0 * math.pi)
    rough = jax.random.uniform(second_key, (LAYERS, 1, CH), jnp.float32, -0.35, 0.35)
    factor = jnp.exp(1.2 * jnp.sin(2.0 * math.pi * 3.0 * channel / CH + phase) + rough)
    base = jnp.clip(jax.random.normal(third_key, (LAYERS, TAPS, CH), jnp.float32), -4.0, 4.0)
    return base * factor / math.sqrt(TAPS)


def steps_of(own_key, shape, shards, smallest, high):
    def one(position, blocks):
        steps = jax.random.uniform(jax.random.fold_in(jax.random.fold_in(own_key, 6), position), (blocks,), jnp.float32, smallest / len(shards), high / len(shards))
        return jnp.repeat(jnp.exp(steps), shape[position] // blocks).reshape((-1,) + (1,) * (len(shape) - position - 1))

    level = one(*shards[0])
    for cut in shards[1:]:
        level = level * one(*cut)
    return level


def scatter_about(own_key, shape, width, limit, cuts=(), held_as=jnp.bfloat16):
    entries = width * jax.random.normal(own_key, shape, jnp.float32)
    if cuts:
        entries = entries * steps_of(own_key, shape, cuts, -0.22, 0.18)
    return jnp.clip(entries, -limit, limit).astype(held_as)


def setup_inputs(seed: int = 0) -> dict:
    keys = jax.random.split(jax.random.key(seed), 11)
    tokens = scatter_about(keys[0], (TOKENS, D), 1.0, 6.0, ((0, 4), (1, 8)))
    pre_gain = jnp.clip(1.0 + 0.18 * jax.random.normal(keys[1], (LAYERS, D), jnp.float32), 0.1, 1.9)
    w_value = scatter_about(keys[2], (LAYERS, D, CH), D ** -0.5, 0.09375, ((1, 4), (2, 8)))
    w_gate = scatter_about(keys[3], (LAYERS, D, CH), D ** -0.5, 0.09375, ((1, 4), (2, 8)))
    conv_taps = draw_conv_taps(jax.random.fold_in(keys[10], 71), 0)
    conv_bias = scatter_about(keys[5], (LAYERS, CH), 0.5, 3.0, ((1, 8),), jnp.float32)
    norm_gain = jnp.clip(1.0 + 0.18 * jax.random.normal(keys[6], (LAYERS, CH), jnp.float32), 0.1, 1.9)
    norm_bias = scatter_about(keys[7], (LAYERS, CH), 0.5, 3.0, ((1, 8),), jnp.float32)
    w_out = scatter_about(keys[8], (LAYERS, CH, D), CH ** -0.5, 0.09375, ((1, 4), (2, 8)))
    post_gain = jnp.clip(1.0 + 0.18 * jax.random.normal(keys[9], (LAYERS, D), jnp.float32), 0.1, 1.9)
    return dict(tokens=tokens, pre_gain=pre_gain, w_value=w_value, w_gate=w_gate, conv_taps=conv_taps, conv_bias=conv_bias, norm_gain=norm_gain, norm_bias=norm_bias, w_out=w_out, post_gain=post_gain)


def reference(tokens, pre_gain, w_value, w_gate, conv_taps, conv_bias, norm_gain, norm_bias, w_out, post_gain):
    stream = tokens
    for layer_index in range(LAYERS):
        full_rows = stream.astype(jnp.float32)
        scale_rows = lax.rsqrt(lax.optimization_barrier(jnp.mean(full_rows * full_rows, axis=-1, keepdims=True)) + 1e-06)
        normed = (full_rows * scale_rows * pre_gain[layer_index]).astype(jnp.bfloat16)
        value_proj = jnp.dot(normed, w_value[layer_index], preferred_element_type=jnp.float32)
        gate_proj = jnp.dot(normed, w_gate[layer_index], preferred_element_type=jnp.float32)
        glu_out = (value_proj * jax.nn.sigmoid(gate_proj)).astype(jnp.bfloat16)
        padded = jnp.concatenate([jnp.zeros((TAPS - 1, CH), jnp.bfloat16), glu_out], axis=0).astype(jnp.float32)
        filtered = jnp.zeros((TOKENS, CH), jnp.float32) + conv_bias[layer_index]
        for tap_index in range(TAPS):
            filtered = filtered + padded[tap_index:tap_index + TOKENS] * conv_taps[layer_index, tap_index]
        centre = lax.optimization_barrier(jnp.sum(filtered, axis=-1)) / CH
        spread = jnp.maximum(lax.optimization_barrier(jnp.sum(filtered * filtered, axis=-1)) / CH - centre * centre, 0.0)
        shaped = (filtered - centre[:, None]) * lax.rsqrt(spread + 1e-05)[:, None]
        mixed = jax.nn.silu(shaped * norm_gain[layer_index] + norm_bias[layer_index]).astype(jnp.bfloat16)
        branch_low = jnp.dot(mixed, w_out[layer_index], preferred_element_type=jnp.float32).astype(jnp.bfloat16)
        branch = lax.optimization_barrier(branch_low).astype(jnp.float32)
        total = lax.optimization_barrier(jnp.sum(branch * branch, axis=-1))
        rescale = lax.rsqrt(total / D + 1e-06)[:, None]
        stream = (stream.astype(jnp.float32) + branch * rescale * post_gain[layer_index]).astype(jnp.bfloat16)
    return stream
```

```python
import functools

import jax
import jax.numpy as jnp
from jax import lax
from jax.experimental import pallas as pl
from jax.experimental.pallas import tpu as pltpu
from jax.sharding import PartitionSpec as P

MESH = pl.DeviceIdType.MESH
LANES = 128
HALVES = 2
AHEAD = 2
ROW_TILE = 64
HALO_ROWS = 32


def gray_of(position, count):
    bits = [(position // 2**k) % 2 for k in range(count.bit_length())]
    return sum(((bits[k] + bits[k + 1]) % 2) * 2**k for k in range(count.bit_length() - 1))


def position_of(index, count):
    bits = [(index // 2**k) % 2 for k in range(count.bit_length() - 1)]
    return sum((sum(bits[k:]) % 2) * 2**k for k in range(count.bit_length() - 1))


def loop(count, body):
    def step(index, carry):
        body(index)
        return carry

    lax.fori_loop(0, count, step, 0)


def remote(src, dst, send_sem, recv_sem, axis, target):
    return pltpu.make_async_remote_copy(
        src_ref=src,
        dst_ref=dst,
        send_sem=send_sem,
        recv_sem=recv_sem,
        device_id={axis: target},
        device_id_type=MESH,
    )


def module_kernel(
    ring,
    count,
    tok_ref,
    pre_ref,
    value_ref,
    gate_ref,
    wout_ref,
    taps_ref,
    bias_ref,
    ngain_ref,
    nbias_ref,
    post_ref,
    out_ref,
    w_all,
    u_all,
    f_all,
    mixed,
    acc,
    padded,
    row_a,
    row_b,
    scale_ref,
    shift_ref,
    stream,
    halo_out,
    halo_in,
    stat_out,
    stat_in,
    params,
    z_up,
    z_down,
    z_recv,
    side_send,
    side_recv,
    ahead_send,
    ahead_recv,
    behind_send,
    behind_recv,
    own_sem,
    stat_send,
    stat_recv,
    par_send,
    par_recv,
    halo_send,
    halo_recv,
):
    layers, depth, width = value_ref.shape
    rows = tok_ref.shape[0]
    model = width * count
    tap_count = taps_ref.shape[1]
    chips = count // 2
    half_rows = rows // HALVES
    strips = width // LANES
    groups = rows // LANES
    half_order = tuple(reversed(range(HALVES)))
    pieces = max(1, min(4, depth // 256))
    piece = depth // pieces
    turns = ring // 2

    me = lax.axis_index("tp")
    z = me // 2
    core = me - 2 * z
    partner = me + 1 - 2 * core
    has_up = z < chips - 1
    has_down = z > 0
    spot = lax.axis_index("sp")
    at = position_of(spot, ring)
    ahead = gray_of((at + 1) % ring, ring)
    behind = gray_of((at + ring - 1) % ring, ring)
    has_next = spot < ring - 1
    has_prev = spot > 0

    barrier = pltpu.get_barrier_semaphore()
    for step in range(1, count):
        pl.semaphore_signal(
            barrier, inc=1, device_id={"tp": lax.rem(me + step, count)}, device_id_type=MESH
        )
    pl.semaphore_signal(barrier, inc=1, device_id={"sp": ahead}, device_id_type=MESH)
    pl.semaphore_signal(barrier, inc=1, device_id={"sp": behind}, device_id_type=MESH)

    @pl.when(has_next)
    def _():
        pl.semaphore_signal(barrier, inc=1, device_id={"sp": spot + 1}, device_id_type=MESH)

    @pl.when(has_prev)
    def _():
        pl.semaphore_signal(barrier, inc=1, device_id={"sp": spot - 1}, device_id_type=MESH)

    pl.semaphore_wait(
        barrier, count + 1 + has_next.astype(jnp.int32) + has_prev.astype(jnp.int32)
    )

    sources = (value_ref, gate_ref, wout_ref)
    chunk_total = 3 * layers * pieces

    def held(chunk, owner, first, size):
        start = owner * depth + (chunk % pieces) * piece + first
        return w_all.at[chunk // pieces, pl.ds(pl.multiple_of(start, size), size), :]

    def ring_copy(chunk, step, sign):
        owner = gray_of((at + ring - sign * step) % ring, ring)
        last = step == turns - 1
        size = piece // 2 if last else piece
        first = piece // 2 if last and sign < 0 else 0
        there = held(chunk, owner, first, size)
        projection = chunk // pieces
        own = sources[projection % 3].at[
            projection // 3, pl.ds((chunk % pieces) * piece + first, size), :
        ]
        sends, recvs, target = (
            (ahead_send, ahead_recv, ahead) if sign > 0 else (behind_send, behind_recv, behind)
        )
        return remote(
            own if step == 0 else there,
            there,
            sends.at[chunk, step],
            recvs.at[chunk, step],
            "sp",
            target,
        )

    def own_copy(chunk):
        projection = chunk // pieces
        return pltpu.make_async_copy(
            sources[projection % 3].at[projection // 3, pl.ds((chunk % pieces) * piece, piece), :],
            held(chunk, spot, 0, piece),
            own_sem.at[chunk],
        )

    def start_chunk(chunk):
        if chunk < chunk_total:
            ring_copy(chunk, 0, 1).start()
            ring_copy(chunk, 0, -1).start()
            own_copy(chunk).start()

    def turn_chunk(chunk):
        for step in range(turns - 1):
            ring_copy(chunk, step, 1).wait_recv()
            ring_copy(chunk, step + 1, 1).start()
            ring_copy(chunk, step, -1).wait_recv()
            ring_copy(chunk, step + 1, -1).start()
        start_chunk(chunk + AHEAD)

    def finish_chunk(chunk):
        ring_copy(chunk, turns - 1, 1).wait_recv()
        ring_copy(chunk, turns - 1, -1).wait_recv()
        own_copy(chunk).wait()

    def stage(q):
        return (u_all if q % 2 == 0 else f_all).at[q // 2]

    def part(q, block, half):
        return stage(q).at[block, pl.ds(half * half_rows, half_rows), :]

    def up(q, chip, half):
        there = part(q, 2 * chip + core, half)
        return remote(
            there, there, z_up.at[q, chip, half], z_recv.at[q, chip, half], "tp", me + 2
        )

    def down(q, chip, half):
        there = part(q, 2 * chip + core, half)
        return remote(
            there, there, z_down.at[q, chip, half], z_recv.at[q, chip, half], "tp", me - 2
        )

    def side(q, chip, half):
        there = part(q, 2 * chip + core, half)
        return remote(
            there, there, side_send.at[q, chip, half], side_recv.at[q, chip, half], "tp", partner
        )

    def side_wait(q, chip, half):
        there = part(q, 2 * chip + 1 - core, half)
        remote(
            there, there, side_send.at[q, chip, half], side_recv.at[q, chip, half], "tp", partner
        ).wait_recv()

    def send_own(q, half):
        @pl.when(has_up)
        def _():
            up(q, z, half).start()

        @pl.when(has_down)
        def _():
            down(q, z, half).start()

        side(q, z, half).start()

    low = z + (2 * z > chips - 1).astype(jnp.int32) * (chips - 1 - 2 * z)
    upward = 1 - 2 * (2 * z > chips - 1).astype(jnp.int32)

    def arrival(index):
        both = (index < 2 * low).astype(jnp.int32)
        paired = z + (index // 2 + 1) * (1 if index % 2 else -1)
        alone = z + (index - low + 1) * upward
        return both * paired + (1 - both) * alone

    def relay(q, index, half):
        chip = arrival(index)
        there = part(q, 2 * chip + core, half)
        remote(
            there, there, z_up.at[q, chip, half], z_recv.at[q, chip, half], "tp", partner
        ).wait_recv()

        @pl.when((chip < z) & has_up)
        def _():
            up(q, chip, half).start()

        @pl.when((chip > z) & has_down)
        def _():
            down(q, chip, half).start()

        side(q, chip, half).start()

    def drain(q):
        def chip_step(chip):
            for half in range(HALVES):
                side(q, chip, half).wait_send()

                @pl.when(has_up & (chip <= z))
                def _():
                    up(q, chip, half).wait_send()

                @pl.when(has_down & (chip >= z))
                def _():
                    down(q, chip, half).wait_send()

        loop(chips, chip_step)

    def stat_copy(event, step):
        return remote(
            stat_out.at[event],
            stat_in.at[event, step - 1],
            stat_send.at[event, step - 1],
            stat_recv.at[event, step - 1],
            "tp",
            lax.rem(me + step, count),
        )

    def pack_rows(event, base, ref):
        for group in range(groups):
            turned = ref[group * LANES : (group + 1) * LANES, :].T
            stat_out[event, base + group : base + group + 1, :] = jnp.sum(
                turned, axis=0, keepdims=True
            )

    def send_stats(event):
        for step in range(1, count):
            stat_copy(event, step).start()

    def total_stats(event):
        total = stat_out[event]
        for step in range(1, count):
            stat_copy(event, step).wait_recv()
            total = total + stat_in[event, step - 1]
        return total

    def spread_rows(ref, packed, base):
        for group in range(groups):
            line = packed[base + group : base + group + 1, :]
            ref[group * LANES : (group + 1) * LANES, :] = jnp.broadcast_to(
                line, (LANES, LANES)
            ).T

    def strip(index):
        return slice(index * LANES, (index + 1) * LANES)

    def tile_at(base, index):
        return pl.ds(pl.multiple_of(base + index * ROW_TILE, ROW_TILE), ROW_TILE)

    half_tiles = half_rows // ROW_TILE

    def emit_u(layer, half, source):
        def body(index):
            at_rows = tile_at(half * half_rows, index)
            values = source(at_rows)
            squares = jnp.zeros((ROW_TILE, LANES), jnp.float32)
            for s in range(strips):
                own = values[:, strip(s)]
                squares = squares + own * own
            row_a[at_rows, :] = squares
            gain = pre_ref[layer : layer + 1, pl.ds(pl.multiple_of(me * width, width), width)]
            u_all[layer, me, at_rows, :] = (values * gain).astype(jnp.bfloat16)

        loop(half_tiles, body)

    column_tile = min(256, width)

    def columns(index):
        return pl.ds(pl.multiple_of(index * column_tile, column_tile), column_tile)

    def project(layer, which, chunk):
        offset = (chunk % pieces) * piece

        def body(index):
            total = None
            for owner in range(ring):
                first = owner * depth + offset
                block, column = first // width, first % width
                product = jnp.dot(
                    u_all[layer, block, :, column : column + piece],
                    w_all[3 * layer + which, first : first + piece, columns(index)],
                    preferred_element_type=jnp.float32,
                )
                total = product if total is None else total + product
            if chunk % pieces == 0:
                acc[which, :, columns(index)] = total
            else:
                acc[which, :, columns(index)] += total

        loop(width // column_tile, body)

    def gated(layer, half):
        def body(index):
            at_rows = tile_at(half * half_rows, index)
            scale = scale_ref[at_rows, :]
            for s in range(strips):
                value = acc[0, at_rows, strip(s)] * scale
                gate = acc[1, at_rows, strip(s)] * scale
                glu = (value * (0.5 * (1.0 + jnp.tanh(0.5 * gate)))).astype(jnp.bfloat16)
                padded[
                    s,
                    pl.ds(
                        pl.multiple_of(HALO_ROWS + half * half_rows + index * ROW_TILE, 8), ROW_TILE
                    ),
                    :,
                ] = glu.astype(jnp.float32)

        loop(half_tiles, body)

    def filter_rows(layer, half):
        def body(index):
            at_rows = tile_at(half * half_rows, index)
            start = half * half_rows + index * ROW_TILE + HALO_ROWS - (tap_count - 1)
            first = jnp.zeros((ROW_TILE, LANES), jnp.float32)
            second = jnp.zeros((ROW_TILE, LANES), jnp.float32)
            for s in range(strips):
                total = jnp.zeros((ROW_TILE, LANES), jnp.float32) + bias_ref[
                    layer : layer + 1, strip(s)
                ]
                for tap in range(tap_count):
                    total = (
                        total
                        + padded[s, pl.ds(start + tap, ROW_TILE), :]
                        * taps_ref[layer, tap : tap + 1, strip(s)]
                    )
                f_all[layer, me, at_rows, strip(s)] = total.astype(jnp.bfloat16)
                first = first + total
                second = second + total * total
            row_a[at_rows, :] = first
            row_b[at_rows, :] = second

        loop(half_tiles, body)

    def mix(layer, chip, half):
        for c in range(2):
            block = 2 * chip + c
            gains = params[block, 2 * layer : 2 * layer + 1, :]
            biases = params[block, 2 * layer + 1 : 2 * layer + 2, :]

            def body(index):
                at_rows = tile_at(half * half_rows, index)
                scale = scale_ref[at_rows, :]
                shift = shift_ref[at_rows, :]
                for s in range(strips):
                    shaped = f_all[layer, block, at_rows, strip(s)].astype(jnp.float32) * scale
                    shaped = (shaped - shift) * gains[:, strip(s)] + biases[:, strip(s)]
                    mixed[block, at_rows, strip(s)] = (
                        shaped * (0.5 * (1.0 + jnp.tanh(0.5 * shaped)))
                    ).astype(jnp.bfloat16)

            loop(half_tiles, body)

    def merge(layer, chip, half, first):
        at_rows = pl.ds(half * half_rows, half_rows)

        def body(index):
            total = None
            for c in range(2):
                block = 2 * chip + c
                product = jnp.dot(
                    mixed[block, at_rows, :],
                    w_all[
                        3 * layer + 2,
                        pl.ds(pl.multiple_of(block * width, width), width),
                        columns(index),
                    ],
                    preferred_element_type=jnp.float32,
                )
                total = product if total is None else total + product
            if first:
                acc[0, at_rows, columns(index)] = total
            else:
                acc[0, at_rows, columns(index)] += total

        loop(width // column_tile, body)

    for chunk in range(AHEAD):
        start_chunk(chunk)

    def from_tokens(at_rows):
        return tok_ref[at_rows, :].astype(jnp.float32)

    for half in half_order:
        emit_u(0, half, from_tokens)
        if half == half_order[0]:
            for layer in range(layers):
                params[me, 2 * layer : 2 * layer + 1, :] = ngain_ref[layer : layer + 1, :]
                params[me, 2 * layer + 1 : 2 * layer + 2, :] = nbias_ref[layer : layer + 1, :]
        send_own(0, half)

    def param_copy(step):
        return remote(
            params.at[me],
            params.at[me],
            par_send.at[step - 1],
            par_recv.at[step - 1],
            "tp",
            lax.rem(me + step, count),
        )

    pack_rows(0, 0, row_a)
    send_stats(0)
    for step in range(1, count):
        param_copy(step).start()

    def halo_copy(layer):
        return remote(
            halo_out.at[layer],
            halo_in.at[layer],
            halo_send.at[layer],
            halo_recv.at[layer],
            "sp",
            lax.rem(spot + 1, ring),
        )

    relays = [(index, half) for index in range(chips - 1) for half in half_order]

    def interleave(q, chunks, after):
        chunks = list(chunks)
        for number, (index, half) in enumerate(relays):
            relay(q, index, half)
            while chunks and len(chunks) * len(relays) > (len(relays) - number - 1) * pieces:
                turn_chunk(chunks.pop(0))
            after(index, half)
        for chunk in chunks:
            turn_chunk(chunk)

    for layer in range(layers):
        base = 3 * layer * pieces
        q = 2 * layer
        event = 3 * layer
        interleave(q, range(base, base + pieces), lambda index, half: None)
        for half in half_order:
            side_wait(q, z, half)
            for index in range(chips - 1):
                side_wait(q, arrival(index), half)
        norm = lax.rsqrt(total_stats(event) / model + 1e-06)
        spread_rows(scale_ref, norm, 0)
        for chunk in range(base, base + pieces):
            finish_chunk(chunk)
            project(layer, 0, chunk)
            turn_chunk(chunk + pieces)
        for chunk in range(base + pieces, base + 2 * pieces):
            finish_chunk(chunk)
            project(layer, 1, chunk)

        for half in half_order:
            gated(layer, half)
            if half == half_order[0]:
                for s in range(strips):
                    halo_out[layer, :, strip(s)] = padded[s, rows : rows + HALO_ROWS, :].astype(
                        jnp.bfloat16
                    )

        @pl.when(has_next)
        def _():
            halo_copy(layer).start()

        for half in half_order:
            if half == 0:

                @pl.when(has_prev)
                def _():
                    halo_copy(layer).wait_recv()
                    for s in range(strips):
                        padded[s, 0:HALO_ROWS, :] = halo_in[layer, :, strip(s)].astype(jnp.float32)

                @pl.when(spot == 0)
                def _():
                    padded[:, 0:HALO_ROWS, :] = jnp.zeros((strips, HALO_ROWS, LANES), jnp.float32)

            filter_rows(layer, half)
            if half == 0:
                pack_rows(event + 1, 0, row_a)
                pack_rows(event + 1, groups, row_b)
                send_stats(event + 1)
            send_own(q + 1, half)

        def normal(layer=layer, event=event):
            totals = total_stats(event + 1) / model
            centre = totals[0:groups, :]
            spread = jnp.maximum(totals[groups : 2 * groups, :] - centre * centre, 0.0)
            inverse = lax.rsqrt(spread + 1e-05)
            spread_rows(scale_ref, inverse, 0)
            spread_rows(shift_ref, centre * inverse, 0)
            if layer == 0:
                for step in range(1, count):
                    param_copy(step).wait_recv()
            for half in half_order:
                side_wait(2 * layer + 1, z, half)
                mix(layer, z, half)

        def ready(index, half, layer=layer, normal=normal):
            q = 2 * layer + 1
            if index == 0 and half == half_order[0]:
                return
            if index == 0:
                normal()
                for again in half_order:
                    side_wait(q, arrival(0), again)
                    mix(layer, arrival(0), again)
                return
            if index < chips - 2:
                side_wait(q, arrival(index), half)
                mix(layer, arrival(index), half)

        interleave(q + 1, range(base + 2 * pieces, base + 3 * pieces), ready)
        for chunk in range(base + 2 * pieces, base + 3 * pieces):
            finish_chunk(chunk)
        for half in half_order:
            merge(layer, z, half, True)
            for index in range(chips - 2):
                merge(layer, arrival(index), half, False)
        for half in half_order:
            chip = arrival(chips - 2)
            side_wait(q + 1, chip, half)
            mix(layer, chip, half)
            merge(layer, chip, half, False)

            def squares(index, half=half):
                at_rows = tile_at(half * half_rows, index)
                total = jnp.zeros((ROW_TILE, LANES), jnp.float32)
                for s in range(strips):
                    own = acc[0, at_rows, strip(s)].astype(jnp.bfloat16).astype(jnp.float32)
                    total = total + own * own
                row_a[at_rows, :] = total

            loop(half_tiles, squares)
        pack_rows(event + 2, 0, row_a)
        send_stats(event + 2)
        spread_rows(scale_ref, lax.rsqrt(total_stats(event + 2) / model + 1e-06), 0)

        def updated(at_rows, layer=layer):
            branch = acc[0, at_rows, :].astype(jnp.bfloat16).astype(jnp.float32)
            scale = jnp.concatenate([scale_ref[at_rows, :]] * strips, axis=1)
            before = (tok_ref if layer == 0 else stream)[at_rows, :].astype(jnp.float32)
            after = before + branch * scale * post_ref[layer : layer + 1, :]
            after = after.astype(jnp.bfloat16)
            if layer + 1 < layers:
                stream[at_rows, :] = after
            else:
                out_ref[at_rows, :] = after
            return after.astype(jnp.float32)

        if layer + 1 < layers:
            for half in half_order:
                emit_u(layer + 1, half, updated)
                send_own(q + 2, half)
            pack_rows(event + 3, 0, row_a)
            send_stats(event + 3)
        else:
            loop(rows // ROW_TILE, lambda index: updated(tile_at(0, index)))

    for chunk in range(chunk_total):
        for step in range(turns):
            ring_copy(chunk, step, 1).wait_send()
            ring_copy(chunk, step, -1).wait_send()
    for q in range(2 * layers):
        drain(q)
    for step in range(1, count):
        for event in range(3 * layers):
            stat_copy(event, step).wait_send()
        param_copy(step).wait_send()

    @pl.when(has_next)
    def _():
        for layer in range(layers):
            halo_copy(layer).wait_send()


def shards(
    tokens, pre_gain, w_value, w_gate, conv_taps, conv_bias, norm_gain, norm_bias, w_out, post_gain
):
    ring = lax.axis_size("sp")
    count = lax.axis_size("tp")
    chips = count // 2
    layers, depth, width = w_value.shape
    rows = tokens.shape[0]
    pieces = max(1, min(4, depth // 256))
    chunks = 3 * layers * pieces
    strips = width // LANES
    stat_rows = max(8, 2 * rows // LANES)
    param_rows = -(-2 * layers // 8) * 8
    vmem = pl.BlockSpec(memory_space=pltpu.VMEM)
    hbm = pl.BlockSpec(memory_space=pl.ANY)
    dma = pltpu.SemaphoreType.DMA
    scratch = [
        pltpu.VMEM((3 * layers, depth * ring, width), jnp.bfloat16),
        pltpu.VMEM((layers, count, rows, width), jnp.bfloat16),
        pltpu.VMEM((layers, count, rows, width), jnp.bfloat16),
        pltpu.VMEM((count, rows, width), jnp.bfloat16),
        pltpu.VMEM((2, rows, width), jnp.float32),
        pltpu.VMEM((strips, HALO_ROWS + rows, LANES), jnp.float32),
        pltpu.VMEM((rows, LANES), jnp.float32),
        pltpu.VMEM((rows, LANES), jnp.float32),
        pltpu.VMEM((rows, LANES), jnp.float32),
        pltpu.VMEM((rows, LANES), jnp.float32),
        pltpu.VMEM((rows, width), jnp.bfloat16),
        pltpu.VMEM((layers, HALO_ROWS, width), jnp.bfloat16),
        pltpu.VMEM((layers, HALO_ROWS, width), jnp.bfloat16),
        pltpu.VMEM((3 * layers, stat_rows, LANES), jnp.float32),
        pltpu.VMEM((3 * layers, count - 1, stat_rows, LANES), jnp.float32),
        pltpu.VMEM((count, param_rows, width), jnp.float32),
    ]
    scratch += [dma((2 * layers, chips, HALVES))] * 5
    scratch += [dma((chunks, ring // 2))] * 4
    scratch += [dma((chunks,))]
    scratch += [dma((3 * layers, count - 1))] * 2
    scratch += [dma((count - 1,))] * 2
    scratch += [dma((layers,))] * 2
    flops = 2 * rows * model_width(tokens, count) * width * 3 * layers
    return pl.pallas_call(
        functools.partial(module_kernel, ring, count),
        out_shape=jax.ShapeDtypeStruct(tokens.shape, tokens.dtype),
        in_specs=[vmem, vmem, hbm, hbm, hbm] + [vmem] * 5,
        out_specs=vmem,
        scratch_shapes=scratch,
        compiler_params=pltpu.CompilerParams(
            collective_id=0, has_side_effects=True, vmem_limit_bytes=63 * 2**20
        ),
        cost_estimate=pl.CostEstimate(flops=flops, bytes_accessed=flops // 512, transcendentals=0),
        name="modules",
    )(
        tokens,
        pre_gain,
        w_value,
        w_gate,
        w_out,
        conv_taps,
        conv_bias,
        norm_gain,
        norm_bias,
        post_gain,
    )


def model_width(tokens, count):
    return tokens.shape[1] * count


def solution(mesh):
    in_specs = (
        P("sp", "tp"),
        P(),
        P(None, "sp", "tp"),
        P(None, "sp", "tp"),
        P(None, None, "tp"),
        P(None, "tp"),
        P(None, "tp"),
        P(None, "tp"),
        P(None, "sp", "tp"),
        P(None, "tp"),
    )
    out_specs = P("sp", "tp")
    return jax.shard_map(shards, mesh=mesh, in_specs=in_specs, out_specs=out_specs, check_vma=False)
```

```python
import functools

import jax
import jax.numpy as jnp
from jax import lax
from jax.experimental import pallas as pl
from jax.experimental.pallas import tpu as pltpu
from jax.sharding import PartitionSpec as P

MESH = pl.DeviceIdType.MESH
LANES = 128
HALVES = 2
AHEAD = 3
ROW_TILE = 64
HALO_ROWS = 32
LATE_TURNS = (0, 0, 1, 3)
OUT_TURNS = (1, 2, 4, 5)
LAST_TURNS = (0, 0, 1, 3)


def gray_of(position, count):
    bits = [(position // 2**k) % 2 for k in range(count.bit_length())]
    return sum(((bits[k] + bits[k + 1]) % 2) * 2**k for k in range(count.bit_length() - 1))


def position_of(index, count):
    bits = [(index // 2**k) % 2 for k in range(count.bit_length() - 1)]
    return sum((sum(bits[k:]) % 2) * 2**k for k in range(count.bit_length() - 1))


def loop(count, body):
    def step(index, carry):
        body(index)
        return carry

    lax.fori_loop(0, count, step, 0)


def remote(src, dst, send_sem, recv_sem, axis, target):
    return pltpu.make_async_remote_copy(
        src_ref=src,
        dst_ref=dst,
        send_sem=send_sem,
        recv_sem=recv_sem,
        device_id={axis: target},
        device_id_type=MESH,
    )


def module_kernel(
    ring,
    count,
    tok_hbm,
    pre_hbm,
    value_ref,
    gate_ref,
    wout_ref,
    taps_hbm,
    bias_hbm,
    ngain_hbm,
    nbias_hbm,
    post_hbm,
    out_ref,
    tok_ref,
    pre_ref,
    taps_ref,
    bias_ref,
    ngain_ref,
    nbias_ref,
    post_ref,
    load_sem,
    tap_rows,
    w_all,
    u_all,
    f_all,
    mixed,
    acc,
    padded,
    row_a,
    row_b,
    scale_ref,
    shift_ref,
    stream,
    last,
    last_sem,
    halo_out,
    halo_in,
    stat_out,
    stat_in,
    params,
    x_all,
    half_out,
    half_in,
    z_up,
    z_down,
    z_recv,
    side_send,
    side_recv,
    ring_send,
    ring_recv,
    sub_send,
    sub_recv,
    own_sem,
    x_send,
    x_recv,
    pass_send,
    pass_recv,
    half_send,
    half_recv,
    stat_send,
    stat_recv,
    par_send,
    par_recv,
    halo_send,
    halo_recv,
):
    layers, depth, width = value_ref.shape
    rows = tok_ref.shape[0]
    model = width * count
    tap_count = taps_ref.shape[0]
    chips = count // 2
    half_rows = rows // HALVES
    strips = width // LANES
    groups = rows // LANES
    half_order = tuple(reversed(range(HALVES)))
    pieces = max(1, min(4, depth // 256))
    piece = depth // pieces
    turns = ring // 2
    group = ring // 2
    group_turns = max(1, group // 2)
    blocks_held = depth // width

    me = lax.axis_index("tp")
    z = me // 2
    core = me - 2 * z
    partner = me + 1 - 2 * core
    has_up = z < chips - 1
    has_down = z > 0
    spot = lax.axis_index("sp")
    at = position_of(spot, ring)
    ahead = gray_of((at + 1) % ring, ring)
    behind = gray_of((at + ring - 1) % ring, ring)
    low_bit = spot % 2
    pair = spot + 1 - 2 * low_bit
    group_at = position_of(spot // 2, group)
    group_ahead = 2 * gray_of((group_at + 1) % group, group) + low_bit
    group_behind = 2 * gray_of((group_at + group - 1) % group, group) + low_bit
    x_way = at % 2
    has_next = spot < ring - 1
    has_prev = spot > 0

    barrier = pltpu.get_barrier_semaphore()
    for step in range(1, count):
        pl.semaphore_signal(
            barrier, inc=1, device_id={"tp": lax.rem(me + step, count)}, device_id_type=MESH
        )
    pl.semaphore_signal(barrier, inc=1, device_id={"sp": ahead}, device_id_type=MESH)
    pl.semaphore_signal(barrier, inc=1, device_id={"sp": behind}, device_id_type=MESH)
    if group > 2:
        for member in (group_ahead, group_behind):
            pl.semaphore_signal(barrier, inc=1, device_id={"sp": member}, device_id_type=MESH)

    @pl.when(has_next)
    def _():
        pl.semaphore_signal(barrier, inc=1, device_id={"sp": spot + 1}, device_id_type=MESH)

    @pl.when(has_prev)
    def _():
        pl.semaphore_signal(barrier, inc=1, device_id={"sp": spot - 1}, device_id_type=MESH)

    loads = [
        pltpu.make_async_copy(source, there, load_sem.at[number])
        for number, (source, there) in enumerate(
            [
                (tok_hbm, tok_ref),
                (pre_hbm, pre_ref),
                (ngain_hbm, ngain_ref),
                (nbias_hbm, nbias_ref),
                (taps_hbm, taps_ref),
                (bias_hbm, bias_ref),
                (post_hbm, post_ref),
            ]
        )
    ]
    for load in loads:
        load.start()

    pl.semaphore_wait(
        barrier,
        count + (3 if group > 2 else 1) + has_next.astype(jnp.int32) + has_prev.astype(jnp.int32)
    )

    sources = (value_ref, gate_ref, wout_ref)
    chunk_total = 3 * layers * pieces

    def held(chunk, owner, first, size):
        start = owner * depth + (chunk % pieces) * piece + first
        return w_all.at[chunk // pieces, pl.ds(pl.multiple_of(start, size), size), :]

    def own_rows(chunk, first, size):
        projection = chunk // pieces
        return sources[projection % 3].at[
            projection // 3, pl.ds((chunk % pieces) * piece + first, size), :
        ]

    def ring_copy(chunk, step, way):
        owner = gray_of((at + ring - (1 - 2 * way) * step) % ring, ring)
        last = step == turns - 1
        size = piece // 2 if last else piece
        there = held(chunk, owner, size * way if last else 0, size)
        return remote(
            own_rows(chunk, 0, size) if step == 0 else there,
            there,
            ring_send.at[way, chunk, step],
            ring_recv.at[way, chunk, step],
            "sp",
            ahead * (1 - way) + behind * way,
        )

    def sub_copy(chunk, step, way):
        owner = 2 * gray_of((group_at + group - (1 - 2 * way) * step) % group, group) + low_bit
        last = step == group_turns - 1
        size = piece // 2 if last else piece
        first = size * way if last else 0
        there = held(chunk, owner, first, size)
        return remote(
            own_rows(chunk, first, size) if step == 0 else there,
            there,
            sub_send.at[way, chunk, step],
            sub_recv.at[way, chunk, step],
            "sp",
            group_behind if way else group_ahead,
        )

    def finish_sub(chunk):
        for step in range(group_turns - 1):
            for way in range(2):
                sub_copy(chunk, step, way).wait_recv()
                sub_copy(chunk, step + 1, way).start()
        for way in range(2):
            sub_copy(chunk, group_turns - 1, way).wait_recv()
        own_copy(chunk).wait()

    def own_copy(chunk):
        projection = chunk // pieces
        return pltpu.make_async_copy(
            sources[projection % 3].at[projection // 3, pl.ds((chunk % pieces) * piece, piece), :],
            held(chunk, spot, 0, piece),
            own_sem.at[chunk],
        )

    started = [3 * pieces]

    def start_until(last):
        while started[0] <= min(last, chunk_total - 1):
            for way in range(2):
                ring_copy(started[0], 0, way).start()
            own_copy(started[0]).start()
            started[0] += 1

    def turn_chunk(chunk, most):
        for step in range(turns - 1):
            for way in range(2):
                ring_copy(chunk, step, way).wait_recv()
                ring_copy(chunk, step + 1, way).start()
        if chunk < 5 * pieces - 1:
            most = min(most, 5 * pieces - 1)
        start_until(min(chunk + AHEAD, most))

    def finish_chunk(chunk):
        for way in range(2):
            ring_copy(chunk, turns - 1, way).wait_recv()
        own_copy(chunk).wait()

    def stage(q):
        return (u_all if q % 2 == 0 else f_all).at[q // 2]

    def part(q, block, half):
        return stage(q).at[block, pl.ds(half * half_rows, half_rows), :]

    def up(q, chip, half):
        there = part(q, 2 * chip + core, half)
        return remote(
            there, there, z_up.at[q, chip, half], z_recv.at[q, chip, half], "tp", me + 2
        )

    def down(q, chip, half):
        there = part(q, 2 * chip + core, half)
        return remote(
            there, there, z_down.at[q, chip, half], z_recv.at[q, chip, half], "tp", me - 2
        )

    def side(q, chip, half):
        there = part(q, 2 * chip + core, half)
        return remote(
            there, there, side_send.at[q, chip, half], side_recv.at[q, chip, half], "tp", partner
        )

    def side_wait(q, chip, half):
        there = part(q, 2 * chip + 1 - core, half)
        remote(
            there, there, side_send.at[q, chip, half], side_recv.at[q, chip, half], "tp", partner
        ).wait_recv()

    def mine(block):
        return (block // blocks_held) % 2 == low_bit

    def x_copy(chip, half):
        block = 2 * chip + core
        return remote(
            part(0, block, half),
            x_all.at[block, pl.ds(half * half_rows, half_rows), :],
            x_send.at[chip, half],
            x_recv.at[chip, half],
            "sp",
            pair,
        )

    def pass_copy(chip, half, block):
        there = x_all.at[block, pl.ds(half * half_rows, half_rows), :]
        return remote(
            there, there, pass_send.at[chip, half], pass_recv.at[chip, half], "tp", partner
        )

    def cross(chip, half):
        @pl.when(mine(2 * chip + core))
        def _():
            x_copy(chip, half).wait_recv()
            pass_copy(chip, half, 2 * chip + core).start()

    def cross_wait(chip, half):
        @pl.when(mine(2 * chip + 1 - core))
        def _():
            pass_copy(chip, half, 2 * chip + 1 - core).wait_recv()

    def half_copy(which, half):
        at_rows = pl.ds(half * half_rows, half_rows)
        return remote(
            half_out.at[which, at_rows, :],
            half_in.at[which, at_rows, :],
            half_send.at[which, half],
            half_recv.at[which, half],
            "sp",
            pair,
        )

    def send_own(q, half):
        if q == 0:

            @pl.when(jnp.logical_not(mine(me)))
            def _():
                x_copy(z, half).start()

        @pl.when(has_up)
        def _():
            up(q, z, half).start()

        @pl.when(has_down)
        def _():
            down(q, z, half).start()

        side(q, z, half).start()

    low = z + (2 * z > chips - 1).astype(jnp.int32) * (chips - 1 - 2 * z)
    upward = 1 - 2 * (2 * z > chips - 1).astype(jnp.int32)

    def arrival(index):
        both = (index < 2 * low).astype(jnp.int32)
        paired = z + (index // 2 + 1) * (1 if index % 2 else -1)
        alone = z + (index - low + 1) * upward
        return both * paired + (1 - both) * alone

    def relay(q, index, half):
        for sign in (-1, 1):
            chip = z + sign * (index + 1)

            @pl.when((chip >= 0) & (chip < chips))
            def _():
                there = part(q, 2 * chip + core, half)
                remote(
                    there, there, z_up.at[q, chip, half], z_recv.at[q, chip, half], "tp", partner
                ).wait_recv()

                if sign < 0:

                    @pl.when(has_up)
                    def _():
                        up(q, chip, half).start()

                else:

                    @pl.when(has_down)
                    def _():
                        down(q, chip, half).start()

                side(q, chip, half).start()
                if q == 0:

                    @pl.when(jnp.logical_not(mine(2 * chip + core)))
                    def _():
                        x_copy(chip, half).start()

    def drain(q):
        def chip_step(chip):
            for half in range(HALVES):
                side(q, chip, half).wait_send()
                if q == 0:
                    for_me = mine(2 * chip + core)

                    @pl.when(for_me)
                    def _():
                        pass_copy(chip, half, 2 * chip + core).wait_send()

                    @pl.when(jnp.logical_not(for_me))
                    def _():
                        x_copy(chip, half).wait_send()

                @pl.when(has_up & (chip <= z))
                def _():
                    up(q, chip, half).wait_send()

                @pl.when(has_down & (chip >= z))
                def _():
                    down(q, chip, half).wait_send()

        loop(chips, chip_step)

    def stat_copy(event, step):
        return remote(
            stat_out.at[event],
            stat_in.at[event, step - 1],
            stat_send.at[event, step - 1],
            stat_recv.at[event, step - 1],
            "tp",
            lax.rem(me + step, count),
        )

    def pack_rows(event, base, ref):
        for group in range(groups):
            turned = ref[group * LANES : (group + 1) * LANES, :].T
            stat_out[event, base + group : base + group + 1, :] = jnp.sum(
                turned, axis=0, keepdims=True
            )

    def send_stats(event):
        for step in range(1, count):
            stat_copy(event, step).start()

    def total_stats(event):
        total = stat_out[event]
        for step in range(1, count):
            stat_copy(event, step).wait_recv()
            total = total + stat_in[event, step - 1]
        return total

    def spread_rows(ref, packed, base):
        for group in range(groups):
            line = packed[base + group : base + group + 1, :]
            ref[group * LANES : (group + 1) * LANES, :] = jnp.broadcast_to(
                line, (LANES, LANES)
            ).T

    def strip(index):
        return slice(index * LANES, (index + 1) * LANES)

    def tile_at(base, index):
        return pl.ds(pl.multiple_of(base + index * ROW_TILE, ROW_TILE), ROW_TILE)

    half_tiles = half_rows // ROW_TILE

    def emit_u(layer, half, source):
        def body(index):
            at_rows = tile_at(half * half_rows, index)
            values = source(at_rows)
            squares = jnp.zeros((ROW_TILE, LANES), jnp.float32)
            for s in range(strips):
                own = values[:, strip(s)]
                squares = squares + own * own
            row_a[at_rows, :] = squares
            gain = pre_ref[layer : layer + 1, pl.ds(pl.multiple_of(me * width, width), width)]
            u_all[layer, me, at_rows, :] = (values * gain).astype(jnp.bfloat16)

        loop(half_tiles, body)

    column_tile = min(256, width)

    def columns(index):
        return pl.ds(pl.multiple_of(index * column_tile, column_tile), column_tile)

    def weigh(projection, block, index):
        rows_of = pl.ds(pl.multiple_of(block * width, width), width)
        return w_all[projection, rows_of, columns(index)]

    def project_part(which, half, source, keep):
        at_rows = pl.ds(half * half_rows, half_rows)

        def body(index):
            total = None
            for member in range(group):
                for inner in range(blocks_held):
                    block = (2 * member + low_bit) * blocks_held + inner
                    product = jnp.dot(
                        source[block, at_rows, :],
                        weigh(which, block, index),
                        preferred_element_type=jnp.float32,
                    )
                    total = product if total is None else total + product
            keep(at_rows, columns(index), total)

        loop(width // column_tile, body)

    def project_other(which, half):
        def keep(at_rows, at_columns, total):
            half_out[which, at_rows, at_columns] = total.astype(jnp.bfloat16)

        project_part(which, half, x_all, keep)
        half_copy(which, half).start()

    def project_mine(which, half):
        def keep(at_rows, at_columns, total):
            acc[which, at_rows, at_columns] = total

        project_part(which, half, u_all.at[0], keep)

    def project_chip(layer, which, chip, half, first):
        at_rows = pl.ds(half * half_rows, half_rows)

        def body(index):
            total = None
            for c in range(2):
                product = jnp.dot(
                    u_all[layer, 2 * chip + c, at_rows, :],
                    weigh(3 * layer + which, 2 * chip + c, index),
                    preferred_element_type=jnp.float32,
                )
                total = product if total is None else total + product
            if first:
                acc[which, at_rows, columns(index)] = total
            else:
                acc[which, at_rows, columns(index)] += total

        loop(width // column_tile, body)

    def gated(layer, half):
        def body(index):
            at_rows = tile_at(half * half_rows, index)
            scale = scale_ref[at_rows, :]
            for s in range(strips):
                value = acc[0, at_rows, strip(s)]
                gate = acc[1, at_rows, strip(s)]
                if layer == 0:
                    value = value + half_in[0, at_rows, strip(s)].astype(jnp.float32)
                    gate = gate + half_in[1, at_rows, strip(s)].astype(jnp.float32)
                value = value * scale
                gate = gate * scale
                glu = (value * (0.5 * (1.0 + jnp.tanh(0.5 * gate)))).astype(jnp.bfloat16)
                padded[
                    s,
                    pl.ds(
                        pl.multiple_of(HALO_ROWS + half * half_rows + index * ROW_TILE, 8), ROW_TILE
                    ),
                    :,
                ] = glu.astype(jnp.float32)

        loop(half_tiles, body)

    def filter_rows(layer, half):
        def body(index):
            at_rows = tile_at(half * half_rows, index)
            start = half * half_rows + index * ROW_TILE + HALO_ROWS - (tap_count - 1)
            first = jnp.zeros((ROW_TILE, LANES), jnp.float32)
            second = jnp.zeros((ROW_TILE, LANES), jnp.float32)
            for s in range(strips):
                total = jnp.zeros((ROW_TILE, LANES), jnp.float32) + bias_ref[
                    layer : layer + 1, strip(s)
                ]
                for tap in range(tap_count):
                    total = (
                        total
                        + padded[s, pl.ds(start + tap, ROW_TILE), :]
                        * tap_rows[layer, tap : tap + 1, strip(s)]
                    )
                f_all[layer, me, at_rows, strip(s)] = total.astype(jnp.bfloat16)
                first = first + total
                second = second + total * total
            row_a[at_rows, :] = first
            row_b[at_rows, :] = second

        loop(half_tiles, body)

    def mix(layer, chip, half):
        for c in range(2):
            block = 2 * chip + c
            gains = params[block, 2 * layer : 2 * layer + 1, :]
            biases = params[block, 2 * layer + 1 : 2 * layer + 2, :]

            def body(index):
                at_rows = tile_at(half * half_rows, index)
                scale = scale_ref[at_rows, :]
                shift = shift_ref[at_rows, :]
                for s in range(strips):
                    shaped = f_all[layer, block, at_rows, strip(s)].astype(jnp.float32) * scale
                    shaped = (shaped - shift) * gains[:, strip(s)] + biases[:, strip(s)]
                    mixed[block, at_rows, strip(s)] = (
                        shaped * (0.5 * (1.0 + jnp.tanh(0.5 * shaped)))
                    ).astype(jnp.bfloat16)

            loop(half_tiles, body)

    def merge(layer, chip, half, first):
        at_rows = pl.ds(half * half_rows, half_rows)

        def body(index):
            total = None
            for c in range(2):
                block = 2 * chip + c
                product = jnp.dot(
                    mixed[block, at_rows, :],
                    weigh(3 * layer + 2, block, index),
                    preferred_element_type=jnp.float32,
                )
                total = product if total is None else total + product
            if first:
                acc[0, at_rows, columns(index)] = total
            else:
                acc[0, at_rows, columns(index)] += total

        loop(width // column_tile, body)

    for chunk in range(2 * pieces):
        for way in range(2):
            sub_copy(chunk, 0, way).start()
        own_copy(chunk).start()
    for load in loads[:4]:
        load.wait()

    def from_tokens(at_rows):
        return tok_ref[at_rows, :].astype(jnp.float32)

    for half in half_order:
        emit_u(0, half, from_tokens)
        if half == half_order[0]:
            for layer in range(layers):
                params[me, 2 * layer : 2 * layer + 1, :] = ngain_ref[layer : layer + 1, :]
                params[me, 2 * layer + 1 : 2 * layer + 2, :] = nbias_ref[layer : layer + 1, :]
        send_own(0, half)

    def param_copy(step):
        return remote(
            params.at[me],
            params.at[me],
            par_send.at[step - 1],
            par_recv.at[step - 1],
            "tp",
            lax.rem(me + step, count),
        )

    for chunk in range(2 * pieces, 3 * pieces):
        ring_copy(chunk, 0, 1 - x_way).start()
        own_copy(chunk).start()
    pack_rows(0, 0, row_a)
    send_stats(0)
    for step in range(1, count):
        param_copy(step).start()

    def result_copy(half):
        at_rows = pl.ds(half * half_rows, half_rows)
        return pltpu.make_async_copy(last.at[at_rows, :], out_ref.at[at_rows, :], last_sem.at[half])

    def halo_copy(layer):
        return remote(
            halo_out.at[layer],
            halo_in.at[layer],
            halo_send.at[layer],
            halo_recv.at[layer],
            "sp",
            lax.rem(spot + 1, ring),
        )

    relays = [(index, half) for index in range(chips - 1) for half in half_order]

    def interleave(q, turns_at, chunks, most, after):
        chunks = list(chunks)
        for number, (index, half) in enumerate(relays):
            for _ in range(turns_at.count(number)):
                if chunks:
                    turn_chunk(chunks.pop(0), most)
            relay(q, index, half)
            after(index, half)
        for chunk in chunks:
            turn_chunk(chunk, most)

    def row_scale(event):
        norm = lax.rsqrt(total_stats(event) / model + 1e-06)
        spread_rows(scale_ref, norm, 0)

    def glu_and_halo(layer, half):
        gated(layer, half)
        if half == half_order[0]:
            for s in range(strips):
                halo_out[layer, :, strip(s)] = padded[s, rows : rows + HALO_ROWS, :].astype(
                    jnp.bfloat16
                )

            @pl.when(has_next)
            def _():
                halo_copy(layer).start()

    first_out = 2 * pieces
    second = 3 * pieces
    midway = 5 * pieces + pieces // 2
    turns_of = (
        range(second, second + pieces),
        range(second + pieces, 5 * pieces),
        range(5 * pieces, 6 * pieces),
    )

    def first_projections():
        crossings = [(z, half) for half in half_order]
        crossings += [(arrival(index), half) for index, half in relays]
        paced = list(range(first_out, second))
        kept = paced[3:]
        paced = paced[:3]

        def pace():
            if paced:
                ring_copy(paced.pop(0), 0, x_way).start()

        pace()
        pace()

        def after(index, half):
            pace()
            if (index, half) != relays[0]:
                cross(*crossings.pop(0))

        interleave(0, (), (), 0, after)
        for half in half_order:
            side_wait(0, z, half)
            for index in range(chips - 1):
                side_wait(0, arrival(index), half)
        row_scale(0)
        for load in loads[4:]:
            load.wait()
        for each in range(layers):
            for tap in range(tap_count):
                tap_rows[each, tap : tap + 1, :] = taps_ref[tap, each : each + 1, :]
        for which in range(2):
            for chunk in range(which * pieces, (which + 1) * pieces):
                finish_sub(chunk)
            for half in half_order:
                if which == 0:
                    while crossings and crossings[0][1] == half or len(crossings) > 1:
                        cross(*crossings.pop(0))
                    for index in range(-1, chips - 1):
                        cross_wait(z if index < 0 else arrival(index), half)
                project_other(which, half)
            if which == 1:
                for chunk in paced + kept:
                    ring_copy(chunk, 0, x_way).start()
            for half in half_order:
                project_mine(which, half)
        for chunk in range(first_out, first_out + pieces // 2):
            turn_chunk(chunk, 0)
        for half in half_order:
            for which in range(2):
                half_copy(which, half).wait_recv()
            glu_and_halo(0, half)
    def later_projections(layer):
        base = 3 * layer * pieces

        def chip_of(index):
            return z if index < 0 else arrival(index)

        def take(which, index, half):
            project_chip(layer, which, chip_of(index), half, index < 0)

        def after(index, half):
            if half == half_order[-1] and index < chips - 2:
                if index == 0:
                    for chunk in range(base, base + pieces):
                        finish_chunk(chunk)
                for done in [-1, 0] if index == 0 else [index]:
                    for each in half_order:
                        side_wait(2 * layer, chip_of(done), each)
                        take(0, done, each)
            if index == chips - 2:
                if half == half_order[0]:
                    for chunk in range(base + pieces, base + 2 * pieces):
                        finish_chunk(chunk)
                    for done in range(-1, chips - 2):
                        for each in half_order:
                            take(1, done, each)
                else:
                    row_scale(3 * layer)
                side_wait(2 * layer, chip_of(index), half)
                take(0, index, half)
                take(1, index, half)

        interleave(2 * layer, LATE_TURNS, turns_of[1], midway - 1, after)
        for half in half_order:
            glu_and_halo(layer, half)
        start_until(midway + AHEAD - 1)

    for layer in range(layers):
        q = 2 * layer
        event = 3 * layer
        base = 3 * layer * pieces
        if layer == 0:
            first_projections()
        else:
            later_projections(layer)

        for half in half_order:
            if half == 0:

                @pl.when(has_prev)
                def _():
                    halo_copy(layer).wait_recv()
                    for s in range(strips):
                        padded[s, 0:HALO_ROWS, :] = halo_in[layer, :, strip(s)].astype(jnp.float32)

                @pl.when(spot == 0)
                def _():
                    padded[:, 0:HALO_ROWS, :] = jnp.zeros((strips, HALO_ROWS, LANES), jnp.float32)

            filter_rows(layer, half)
            if half == 0:
                pack_rows(event + 1, 0, row_a)
                pack_rows(event + 1, groups, row_b)
                send_stats(event + 1)
            send_own(q + 1, half)

        if layer == 0:
            for chunk in range(first_out + pieces // 2, second):
                turn_chunk(chunk, midway - 1)

        def normal(layer=layer, event=event):
            totals = total_stats(event + 1) / model
            centre = totals[0:groups, :]
            spread = jnp.maximum(totals[groups : 2 * groups, :] - centre * centre, 0.0)
            inverse = lax.rsqrt(spread + 1e-05)
            spread_rows(scale_ref, inverse, 0)
            spread_rows(shift_ref, centre * inverse, 0)
            if layer == 0:
                for step in range(1, count):
                    param_copy(step).wait_recv()
            for half in half_order:
                side_wait(2 * layer + 1, z, half)
                mix(layer, z, half)

        def ready(index, half, layer=layer, normal=normal):
            q = 2 * layer + 1
            if index == 0 and half == half_order[0]:
                return
            if index == 0:
                normal()
                for again in half_order:
                    side_wait(q, arrival(0), again)
                    mix(layer, arrival(0), again)
                return
            if index == chips - 2 and half == half_order[0]:
                for chunk in range((3 * layer + 2) * pieces, (3 * layer + 3) * pieces):
                    finish_chunk(chunk)
                for each in half_order:
                    for done in range(-1, chips - 2):
                        merge(layer, z if done < 0 else arrival(done), each, done < 0)
            side_wait(q, arrival(index), half)
            mix(layer, arrival(index), half)
            if index == chips - 2:
                merge(layer, arrival(index), half, False)

        interleave(
            q + 1,
            LAST_TURNS if layer else OUT_TURNS,
            turns_of[2] if layer else turns_of[0],
            chunk_total if layer else midway - 1,
            ready,
        )
        for half in half_order:
            def squares(index, half=half):
                at_rows = tile_at(half * half_rows, index)
                total = jnp.zeros((ROW_TILE, LANES), jnp.float32)
                for s in range(strips):
                    own = acc[0, at_rows, strip(s)].astype(jnp.bfloat16).astype(jnp.float32)
                    total = total + own * own
                row_a[at_rows, :] = total

            loop(half_tiles, squares)
        pack_rows(event + 2, 0, row_a)
        send_stats(event + 2)
        spread_rows(scale_ref, lax.rsqrt(total_stats(event + 2) / model + 1e-06), 0)

        def updated(at_rows, layer=layer):
            branch = acc[0, at_rows, :].astype(jnp.bfloat16).astype(jnp.float32)
            scale = jnp.concatenate([scale_ref[at_rows, :]] * strips, axis=1)
            before = (tok_ref if layer == 0 else stream)[at_rows, :].astype(jnp.float32)
            after = before + branch * scale * post_ref[layer : layer + 1, :]
            after = after.astype(jnp.bfloat16)
            if layer + 1 < layers:
                stream[at_rows, :] = after
            else:
                last[at_rows, :] = after
            return after.astype(jnp.float32)

        if layer + 1 < layers:
            for half in half_order:
                emit_u(layer + 1, half, updated)
                send_own(q + 2, half)
            pack_rows(event + 3, 0, row_a)
            send_stats(event + 3)
        else:
            for half in half_order:
                loop(half_tiles, lambda index, half=half: updated(tile_at(half * half_rows, index)))
                result_copy(half).start()

    for way in range(2):
        for chunk in range(2 * pieces):
            for step in range(group_turns):
                sub_copy(chunk, step, way).wait_send()
        for chunk in range(2 * pieces, chunk_total):
            for step in range(turns):
                ring_copy(chunk, step, way).wait_send()
    for which in range(2):
        for half in range(HALVES):
            half_copy(which, half).wait_send()
    for q in range(2 * layers):
        drain(q)
    for step in range(1, count):
        for event in range(3 * layers):
            stat_copy(event, step).wait_send()
        param_copy(step).wait_send()

    @pl.when(has_next)
    def _():
        for layer in range(layers):
            halo_copy(layer).wait_send()

    for half in half_order:
        result_copy(half).wait()


def shards(
    tokens, pre_gain, w_value, w_gate, conv_taps, conv_bias, norm_gain, norm_bias, w_out, post_gain
):
    ring = lax.axis_size("sp")
    count = lax.axis_size("tp")
    chips = count // 2
    layers, depth, width = w_value.shape
    rows = tokens.shape[0]
    pieces = max(1, min(4, depth // 256))
    chunks = 3 * layers * pieces
    strips = width // LANES
    stat_rows = max(8, 2 * rows // LANES)
    param_rows = -(-2 * layers // 8) * 8
    hbm = pl.BlockSpec(memory_space=pl.ANY)
    dma = pltpu.SemaphoreType.DMA
    taps = jnp.transpose(conv_taps, (1, 0, 2))
    loaded = [tokens, pre_gain, taps, conv_bias, norm_gain, norm_bias, post_gain]
    scratch = [pltpu.VMEM(array.shape, array.dtype) for array in loaded]
    scratch += [dma((len(loaded),))]
    scratch += [pltpu.VMEM(conv_taps.shape, conv_taps.dtype)]
    scratch += [
        pltpu.VMEM((3 * layers, depth * ring, width), jnp.bfloat16),
        pltpu.VMEM((layers, count, rows, width), jnp.bfloat16),
        pltpu.VMEM((layers, count, rows, width), jnp.bfloat16),
        pltpu.VMEM((count, rows, width), jnp.bfloat16),
        pltpu.VMEM((2, rows, width), jnp.float32),
        pltpu.VMEM((strips, HALO_ROWS + rows, LANES), jnp.float32),
        pltpu.VMEM((rows, LANES), jnp.float32),
        pltpu.VMEM((rows, LANES), jnp.float32),
        pltpu.VMEM((rows, LANES), jnp.float32),
        pltpu.VMEM((rows, LANES), jnp.float32),
        pltpu.VMEM((rows, width), jnp.bfloat16),
        pltpu.VMEM((rows, width), jnp.bfloat16),
        dma((HALVES,)),
        pltpu.VMEM((layers, HALO_ROWS, width), jnp.bfloat16),
        pltpu.VMEM((layers, HALO_ROWS, width), jnp.bfloat16),
        pltpu.VMEM((3 * layers, stat_rows, LANES), jnp.float32),
        pltpu.VMEM((3 * layers, count - 1, stat_rows, LANES), jnp.float32),
        pltpu.VMEM((count, param_rows, width), jnp.float32),
        pltpu.VMEM((count, rows, width), jnp.bfloat16),
        pltpu.VMEM((2, rows, width), jnp.bfloat16),
        pltpu.VMEM((2, rows, width), jnp.bfloat16),
    ]
    scratch += [dma((2 * layers, chips, HALVES))] * 5
    scratch += [dma((2, chunks, ring // 2))] * 2
    scratch += [dma((2, 2 * pieces, max(1, ring // 4)))] * 2
    scratch += [dma((chunks,))]
    scratch += [dma((chips, HALVES))] * 4
    scratch += [dma((2, HALVES))] * 2
    scratch += [dma((3 * layers, count - 1))] * 2
    scratch += [dma((count - 1,))] * 2
    scratch += [dma((layers,))] * 2
    flops = 2 * rows * model_width(tokens, count) * width * 3 * layers
    return pl.pallas_call(
        functools.partial(module_kernel, ring, count),
        out_shape=jax.ShapeDtypeStruct(tokens.shape, tokens.dtype),
        in_specs=[hbm] * 10,
        out_specs=hbm,
        scratch_shapes=scratch,
        compiler_params=pltpu.CompilerParams(
            collective_id=0, has_side_effects=True, vmem_limit_bytes=63 * 2**20
        ),
        cost_estimate=pl.CostEstimate(flops=flops, bytes_accessed=flops // 512, transcendentals=0),
        name="modules",
    )(
        tokens,
        pre_gain,
        w_value,
        w_gate,
        w_out,
        taps,
        conv_bias,
        norm_gain,
        norm_bias,
        post_gain,
    )


def model_width(tokens, count):
    return tokens.shape[1] * count


def solution(mesh):
    in_specs = (
        P("sp", "tp"),
        P(),
        P(None, "sp", "tp"),
        P(None, "sp", "tp"),
        P(None, None, "tp"),
        P(None, "tp"),
        P(None, "tp"),
        P(None, "tp"),
        P(None, "sp", "tp"),
        P(None, "tp"),
    )
    out_specs = P("sp", "tp")
    return jax.shard_map(shards, mesh=mesh, in_specs=in_specs, out_specs=out_specs, check_vma=False)
```

```python
import functools

import jax
import jax.numpy as jnp
from jax import lax
from jax.experimental import pallas as pl
from jax.experimental.pallas import tpu as pltpu
from jax.sharding import PartitionSpec as P

MESH = pl.DeviceIdType.MESH
LANES = 128
HALVES = 2
AHEAD = 3
TILE_MOST = 112
HALO_ROWS = 32
LATE_TURNS = (0, 1, 3, 5)
OUT_TURNS = (2, 3, 4)
LAST_TURNS = (0, 1, 2, 4)


def gray_of(position, count):
    bits = [(position // 2**k) % 2 for k in range(count.bit_length())]
    return sum(((bits[k] + bits[k + 1]) % 2) * 2**k for k in range(count.bit_length() - 1))


def position_of(index, count):
    bits = [(index // 2**k) % 2 for k in range(count.bit_length() - 1)]
    return sum((sum(bits[k:]) % 2) * 2**k for k in range(count.bit_length() - 1))


def loop(count, body):
    def step(index, carry):
        body(index)
        return carry

    lax.fori_loop(0, count, step, 0)


def remote(src, dst, send_sem, recv_sem, axis, target):
    return pltpu.make_async_remote_copy(
        src_ref=src,
        dst_ref=dst,
        send_sem=send_sem,
        recv_sem=recv_sem,
        device_id={axis: target},
        device_id_type=MESH,
    )


def module_kernel(
    ring,
    count,
    tok_hbm,
    pre_hbm,
    value_ref,
    gate_ref,
    wout_ref,
    taps_hbm,
    bias_hbm,
    ngain_hbm,
    nbias_hbm,
    post_hbm,
    out_ref,
    tok_ref,
    pre_ref,
    taps_ref,
    bias_ref,
    ngain_ref,
    nbias_ref,
    post_ref,
    load_sem,
    tap_rows,
    w_all,
    u_all,
    f_all,
    mixed,
    acc,
    padded,
    row_a,
    row_b,
    scale_ref,
    shift_ref,
    stream,
    last,
    last_sem,
    halo_out,
    halo_in,
    stat_out,
    stat_in,
    params,
    x_all,
    half_out,
    half_in,
    z_up,
    z_down,
    z_recv,
    side_send,
    side_recv,
    ring_send,
    ring_recv,
    sub_send,
    sub_recv,
    own_sem,
    x_send,
    x_recv,
    pass_send,
    pass_recv,
    half_send,
    half_recv,
    stat_send,
    stat_recv,
    par_send,
    par_recv,
    halo_send,
    halo_recv,
):
    layers, depth, width = value_ref.shape
    rows = tok_ref.shape[0]
    model = width * count
    tap_count = taps_ref.shape[0]
    chips = count // 2
    strips = width // LANES
    groups = rows // LANES
    half_order = tuple(reversed(range(HALVES)))
    pieces = max(1, min(4, depth // 256))
    piece = depth // pieces
    turns = ring // 2
    group = ring // 2
    group_turns = max(1, group // 2)
    blocks_held = depth // width

    def bounds(q, half):
        split = rows // 2 - HALO_ROWS * (layers - (q + 1) // 2)
        return (split, rows - split) if half else (0, split)

    def rows_of(q, half):
        start, size = bounds(q, half)
        return pl.ds(start, size)

    def groups_of(q, half):
        start, size = bounds(q, half)
        return start // LANES, -(-(start + size) // LANES)

    def tiles(q, half, body):
        start, size = bounds(q, half)
        tile = max(t for t in range(16, TILE_MOST + 1, 16) if size % t == 0)
        loop(size // tile, lambda index: body(pl.multiple_of(start + index * tile, 16), tile))

    me = lax.axis_index("tp")
    z = me // 2
    core = me - 2 * z
    partner = me + 1 - 2 * core
    has_up = z < chips - 1
    has_down = z > 0
    spot = lax.axis_index("sp")
    at = position_of(spot, ring)
    ahead = gray_of((at + 1) % ring, ring)
    behind = gray_of((at + ring - 1) % ring, ring)
    low_bit = spot % 2
    pair = spot + 1 - 2 * low_bit
    group_at = position_of(spot // 2, group)
    group_ahead = 2 * gray_of((group_at + 1) % group, group) + low_bit
    group_behind = 2 * gray_of((group_at + group - 1) % group, group) + low_bit
    x_way = at % 2
    has_next = spot < ring - 1
    has_prev = spot > 0

    barrier = pltpu.get_barrier_semaphore()
    for step in range(1, count):
        pl.semaphore_signal(
            barrier, inc=1, device_id={"tp": lax.rem(me + step, count)}, device_id_type=MESH
        )
    pl.semaphore_signal(barrier, inc=1, device_id={"sp": ahead}, device_id_type=MESH)
    pl.semaphore_signal(barrier, inc=1, device_id={"sp": behind}, device_id_type=MESH)
    if group > 2:
        for member in (group_ahead, group_behind):
            pl.semaphore_signal(barrier, inc=1, device_id={"sp": member}, device_id_type=MESH)

    @pl.when(has_next)
    def _():
        pl.semaphore_signal(barrier, inc=1, device_id={"sp": spot + 1}, device_id_type=MESH)

    @pl.when(has_prev)
    def _():
        pl.semaphore_signal(barrier, inc=1, device_id={"sp": spot - 1}, device_id_type=MESH)

    loads = [
        pltpu.make_async_copy(source, there, load_sem.at[number])
        for number, (source, there) in enumerate(
            [
                (tok_hbm, tok_ref),
                (pre_hbm, pre_ref),
                (ngain_hbm, ngain_ref),
                (nbias_hbm, nbias_ref),
                (taps_hbm, taps_ref),
                (bias_hbm, bias_ref),
                (post_hbm, post_ref),
            ]
        )
    ]
    for load in loads:
        load.start()

    pl.semaphore_wait(
        barrier,
        count + (3 if group > 2 else 1) + has_next.astype(jnp.int32) + has_prev.astype(jnp.int32)
    )

    sources = (value_ref, gate_ref, wout_ref)
    chunk_total = 3 * layers * pieces

    def held(chunk, owner, first, size):
        start = owner * depth + (chunk % pieces) * piece + first
        return w_all.at[chunk // pieces, pl.ds(pl.multiple_of(start, size), size), :]

    def own_rows(chunk, first, size):
        projection = chunk // pieces
        return sources[projection % 3].at[
            projection // 3, pl.ds((chunk % pieces) * piece + first, size), :
        ]

    def ring_copy(chunk, step, way):
        owner = gray_of((at + ring - (1 - 2 * way) * step) % ring, ring)
        last = step == turns - 1
        size = piece // 2 if last else piece
        there = held(chunk, owner, size * way if last else 0, size)
        return remote(
            own_rows(chunk, 0, size) if step == 0 else there,
            there,
            ring_send.at[chunk - 2 * pieces],
            ring_recv.at[chunk - 2 * pieces, step],
            "sp",
            ahead * (1 - way) + behind * way,
        )

    def sub_copy(chunk, step, way):
        owner = 2 * gray_of((group_at + group - (1 - 2 * way) * step) % group, group) + low_bit
        last = step == group_turns - 1
        size = piece // 2 if last else piece
        first = size * way if last else 0
        there = held(chunk, owner, first, size)
        return remote(
            own_rows(chunk, first, size) if step == 0 else there,
            there,
            sub_send.at[0],
            sub_recv.at[way, chunk, step],
            "sp",
            group_behind if way else group_ahead,
        )

    def finish_sub(chunk):
        for step in range(group_turns - 1):
            for way in range(2):
                sub_copy(chunk, step, way).wait_recv()
                sub_copy(chunk, step + 1, way).start()
        for way in range(2):
            sub_copy(chunk, group_turns - 1, way).wait_recv()
        if chunk % pieces == 0:
            own_copy(chunk // pieces).wait()

    def own_copy(projection):
        return pltpu.make_async_copy(
            sources[projection % 3].at[projection // 3],
            w_all.at[projection, pl.ds(pl.multiple_of(spot * depth, depth), depth), :],
            own_sem.at[projection],
        )

    def await_bytes(ref, sem):
        pltpu.make_async_copy(ref, ref, sem).wait()

    def ring_arrived(chunk, step):
        size = 2 * piece if step < turns - 1 else piece
        await_bytes(w_all.at[0, 0:size, :], ring_recv.at[chunk - 2 * pieces, step])

    started = [3 * pieces]

    def start_until(last):
        while started[0] <= min(last, chunk_total - 1):
            for way in range(2):
                ring_copy(started[0], 0, way).start()
            started[0] += 1

    def turn_chunk(chunk, most):
        for step in range(turns - 1):
            ring_arrived(chunk, step)
            for way in range(2):
                ring_copy(chunk, step + 1, way).start()
        if chunk < 5 * pieces - 1:
            most = min(most, 5 * pieces - 1)
        start_until(min(chunk + AHEAD, most))

    def finish_chunk(chunk):
        ring_arrived(chunk, turns - 1)
        if chunk % pieces == 0:
            own_copy(chunk // pieces).wait()

    def stage(q):
        return (u_all if q % 2 == 0 else f_all).at[q // 2]

    def part(q, block, half):
        return stage(q).at[block, rows_of(q, half), :]

    def up(q, chip, half):
        there = part(q, 2 * chip + core, half)
        return remote(
            there, there, z_up.at[q], z_recv.at[q, chip, half], "tp", me + 2
        )

    def down(q, chip, half):
        there = part(q, 2 * chip + core, half)
        return remote(
            there, there, z_down.at[q], z_recv.at[q, chip, half], "tp", me - 2
        )

    def side(q, chip, half):
        there = part(q, 2 * chip + core, half)
        return remote(
            there, there, side_send.at[q], side_recv.at[q, chip, half], "tp", partner
        )

    def side_wait(q, chip, half):
        there = part(q, 2 * chip + 1 - core, half)
        remote(
            there, there, side_send.at[q], side_recv.at[q, chip, half], "tp", partner
        ).wait_recv()

    def mine(block):
        return (block // blocks_held) % 2 == low_bit

    def x_copy(chip, half):
        block = 2 * chip + core
        return remote(
            part(0, block, half),
            x_all.at[block, rows_of(0, half), :],
            x_send.at[chip, half],
            x_recv.at[chip, half],
            "sp",
            pair,
        )

    def pass_copy(chip, half, block):
        there = x_all.at[block, rows_of(0, half), :]
        return remote(
            there, there, pass_send.at[chip, half], pass_recv.at[chip, half], "tp", partner
        )

    def cross(chip, half):
        @pl.when(mine(2 * chip + core))
        def _():
            x_copy(chip, half).wait_recv()
            pass_copy(chip, half, 2 * chip + core).start()

    def cross_wait(chip, half):
        @pl.when(mine(2 * chip + 1 - core))
        def _():
            pass_copy(chip, half, 2 * chip + 1 - core).wait_recv()

    def half_copy(which, half):
        at_rows = rows_of(0, half)
        return remote(
            half_out.at[which, at_rows, :],
            half_in.at[which, at_rows, :],
            half_send.at[which, half],
            half_recv.at[which, half],
            "sp",
            pair,
        )

    def send_own(q, half):
        if q == 0:

            @pl.when(jnp.logical_not(mine(me)))
            def _():
                x_copy(z, half).start()

        @pl.when(has_up)
        def _():
            up(q, z, half).start()

        @pl.when(has_down)
        def _():
            down(q, z, half).start()

        side(q, z, half).start()

    low = z + (2 * z > chips - 1).astype(jnp.int32) * (chips - 1 - 2 * z)
    upward = 1 - 2 * (2 * z > chips - 1).astype(jnp.int32)

    def arrival(index):
        both = (index < 2 * low).astype(jnp.int32)
        paired = z + (index // 2 + 1) * (1 if index % 2 else -1)
        alone = z + (index - low + 1) * upward
        return both * paired + (1 - both) * alone

    def relay(q, index, half):
        for sign in (-1, 1):
            chip = z + sign * (index + 1)

            @pl.when((chip >= 0) & (chip < chips))
            def _():
                there = part(q, 2 * chip + core, half)
                remote(
                    there, there, z_up.at[q], z_recv.at[q, chip, half], "tp", partner
                ).wait_recv()

                if sign < 0:

                    @pl.when(has_up)
                    def _():
                        up(q, chip, half).start()

                else:

                    @pl.when(has_down)
                    def _():
                        down(q, chip, half).start()

                side(q, chip, half).start()
                if q == 0:

                    @pl.when(jnp.logical_not(mine(2 * chip + core)))
                    def _():
                        x_copy(chip, half).start()

    def drain(q):
        await_bytes(stage(q).at[0:chips], side_send.at[q])
        for chip in range(chips):

            @pl.when(has_up & (z == chip))
            def _():
                await_bytes(stage(q).at[0 : chip + 1], z_up.at[q])

            @pl.when(has_down & (z == chip))
            def _():
                await_bytes(stage(q).at[0 : chips - chip], z_down.at[q])

        if q == 0:
            for chip in range(chips):
                for half in range(HALVES):

                    @pl.when(mine(2 * chip + core))
                    def _():
                        pass_copy(chip, half, 2 * chip + core).wait_send()

                    @pl.when(jnp.logical_not(mine(2 * chip + core)))
                    def _():
                        x_copy(chip, half).wait_send()

    def stat_copy(event, step):
        return remote(
            stat_out.at[event],
            stat_in.at[event, step - 1],
            stat_send.at[0],
            stat_recv.at[event, step - 1],
            "tp",
            lax.rem(me + step, count),
        )

    def pack_rows(event, base, ref, first=0, last=groups):
        for group in range(first, last):
            turned = ref[group * LANES : (group + 1) * LANES, :].T
            stat_out[event, base + group : base + group + 1, :] = jnp.sum(
                turned, axis=0, keepdims=True
            )

    def send_stats(event):
        for step in range(1, count):
            stat_copy(event, step).start()

    def total_stats(event):
        total = stat_out[event]
        for step in range(1, count):
            stat_copy(event, step).wait_recv()
            total = total + stat_in[event, step - 1]
        return total

    def spread_rows(ref, packed, base, first=0, last=groups):
        for group in range(first, last):
            line = packed[base + group : base + group + 1, :]
            ref[group * LANES : (group + 1) * LANES, :] = jnp.broadcast_to(
                line, (LANES, LANES)
            ).T

    def strip(index):
        return slice(index * LANES, (index + 1) * LANES)

    def emit_u(layer, half, source):
        def body(start, tile):
            at_rows = pl.ds(start, tile)
            values = source(at_rows)
            squares = jnp.zeros((tile, LANES), jnp.float32)
            for s in range(strips):
                own = values[:, strip(s)]
                squares = squares + own * own
            row_a[at_rows, :] = squares
            gain = pre_ref[layer : layer + 1, pl.ds(pl.multiple_of(me * width, width), width)]
            u_all[layer, me, at_rows, :] = (values * gain).astype(jnp.bfloat16)

        tiles(2 * layer, half, body)

    column_tile = min(256, width)

    def columns(index):
        return pl.ds(pl.multiple_of(index * column_tile, column_tile), column_tile)

    def weigh(projection, block, index):
        at_block = pl.ds(pl.multiple_of(block * width, width), width)
        return w_all[projection, at_block, columns(index)]

    def project_part(which, half, source, keep):
        at_rows = rows_of(0, half)

        def body(index):
            total = None
            for member in range(group):
                for inner in range(blocks_held):
                    block = (2 * member + low_bit) * blocks_held + inner
                    product = jnp.dot(
                        source[block, at_rows, :],
                        weigh(which, block, index),
                        preferred_element_type=jnp.float32,
                    )
                    total = product if total is None else total + product
            keep(at_rows, columns(index), total)

        loop(width // column_tile, body)

    def project_other(which, half):
        def keep(at_rows, at_columns, total):
            half_out[which, at_rows, at_columns] = total.astype(jnp.bfloat16)

        project_part(which, half, x_all, keep)
        half_copy(which, half).start()

    def project_mine(which, half):
        def keep(at_rows, at_columns, total):
            acc[which, at_rows, at_columns] = total

        project_part(which, half, u_all.at[0], keep)

    def project_chip(layer, which, chip, half, first):
        at_rows = rows_of(2 * layer, half)

        def body(index):
            total = None
            for c in range(2):
                product = jnp.dot(
                    u_all[layer, 2 * chip + c, at_rows, :],
                    weigh(3 * layer + which, 2 * chip + c, index),
                    preferred_element_type=jnp.float32,
                )
                total = product if total is None else total + product
            if first:
                acc[which, at_rows, columns(index)] = total
            else:
                acc[which, at_rows, columns(index)] += total

        loop(width // column_tile, body)

    def project_chunk(layer, which, chunk, at_rows):
        offset = (chunk % pieces) * piece

        def body(index):
            total = None
            for owner in range(ring):
                first = owner * depth + offset
                product = jnp.dot(
                    u_all[layer, first // width, at_rows, first % width : first % width + piece],
                    w_all[3 * layer + which, first : first + piece, columns(index)],
                    preferred_element_type=jnp.float32,
                )
                total = product if total is None else total + product
            if chunk % pieces == 0:
                acc[which, at_rows, columns(index)] = total
            else:
                acc[which, at_rows, columns(index)] += total

        loop(width // column_tile, body)

    def gated(layer, half):
        def body(start, tile):
            at_rows = pl.ds(start, tile)
            scale = scale_ref[at_rows, :]
            for s in range(strips):
                value = acc[0, at_rows, strip(s)]
                gate = acc[1, at_rows, strip(s)]
                if layer == 0:
                    value = value + half_in[0, at_rows, strip(s)].astype(jnp.float32)
                    gate = gate + half_in[1, at_rows, strip(s)].astype(jnp.float32)
                value = value * scale
                gate = gate * scale
                glu = (value * (0.5 * (1.0 + jnp.tanh(0.5 * gate)))).astype(jnp.bfloat16)
                padded[s, pl.ds(pl.multiple_of(HALO_ROWS + start, 8), tile), :] = glu.astype(
                    jnp.float32
                )

        tiles(2 * layer, half, body)

    def filter_rows(layer, half):
        def body(start, tile):
            at_rows = pl.ds(start, tile)
            oldest = start + HALO_ROWS - (tap_count - 1)
            first = jnp.zeros((tile, LANES), jnp.float32)
            second = jnp.zeros((tile, LANES), jnp.float32)
            for s in range(strips):
                total = jnp.zeros((tile, LANES), jnp.float32) + bias_ref[
                    layer : layer + 1, strip(s)
                ]
                for tap in range(tap_count):
                    total = (
                        total
                        + padded[s, pl.ds(oldest + tap, tile), :]
                        * tap_rows[layer, tap : tap + 1, strip(s)]
                    )
                f_all[layer, me, at_rows, strip(s)] = total.astype(jnp.bfloat16)
                first = first + total
                second = second + total * total
            row_a[at_rows, :] = first
            row_b[at_rows, :] = second

        tiles(2 * layer + 1, half, body)

    def mix(layer, chip, half):
        for c in range(2):
            block = 2 * chip + c
            gains = params[block, 2 * layer : 2 * layer + 1, :]
            biases = params[block, 2 * layer + 1 : 2 * layer + 2, :]

            def body(start, tile):
                at_rows = pl.ds(start, tile)
                scale = scale_ref[at_rows, :]
                shift = shift_ref[at_rows, :]
                for s in range(strips):
                    shaped = f_all[layer, block, at_rows, strip(s)].astype(jnp.float32) * scale
                    shaped = (shaped - shift) * gains[:, strip(s)] + biases[:, strip(s)]
                    mixed[block, at_rows, strip(s)] = (
                        shaped * (0.5 * (1.0 + jnp.tanh(0.5 * shaped)))
                    ).astype(jnp.bfloat16)

            tiles(2 * layer + 1, half, body)

    def merge(layer, chip, half, first):
        at_rows = rows_of(2 * layer + 1, half)

        def body(index):
            total = None
            for c in range(2):
                block = 2 * chip + c
                product = jnp.dot(
                    mixed[block, at_rows, :],
                    weigh(3 * layer + 2, block, index),
                    preferred_element_type=jnp.float32,
                )
                total = product if total is None else total + product
            if first:
                acc[0, at_rows, columns(index)] = total
            else:
                acc[0, at_rows, columns(index)] += total

        loop(width // column_tile, body)

    for chunk in range(2 * pieces):
        for way in range(2):
            sub_copy(chunk, 0, way).start()
    for load in loads[:4]:
        load.wait()

    def from_tokens(at_rows):
        return tok_ref[at_rows, :].astype(jnp.float32)

    for half in half_order:
        emit_u(0, half, from_tokens)
        if half == half_order[0]:
            for layer in range(layers):
                params[me, 2 * layer : 2 * layer + 1, :] = ngain_ref[layer : layer + 1, :]
                params[me, 2 * layer + 1 : 2 * layer + 2, :] = nbias_ref[layer : layer + 1, :]
        send_own(0, half)

    def param_copy(step):
        return remote(
            params.at[me],
            params.at[me],
            par_send.at[0],
            par_recv.at[step - 1],
            "tp",
            lax.rem(me + step, count),
        )

    for chunk in range(2 * pieces, 3 * pieces):
        ring_copy(chunk, 0, 1 - x_way).start()
    for projection in range(3 * layers):
        own_copy(projection).start()
    pack_rows(0, 0, row_a)
    send_stats(0)
    for step in range(1, count):
        param_copy(step).start()

    def result_copy(half):
        at_rows = rows_of(2 * layers - 1, half)
        return pltpu.make_async_copy(last.at[at_rows, :], out_ref.at[at_rows, :], last_sem.at[half])

    def halo_copy(layer):
        return remote(
            halo_out.at[layer],
            halo_in.at[layer],
            halo_send.at[layer],
            halo_recv.at[layer],
            "sp",
            lax.rem(spot + 1, ring),
        )

    relays = [(index, half) for index in range(chips - 1) for half in half_order]

    def interleave(q, turns_at, chunks, most, after):
        chunks = list(chunks)
        for number, (index, half) in enumerate(relays):
            for _ in range(turns_at.count(number)):
                if chunks:
                    turn_chunk(chunks.pop(0), most)
            relay(q, index, half)
            after(index, half)
        for chunk in chunks:
            turn_chunk(chunk, most)

    def row_scale(event):
        norm = lax.rsqrt(total_stats(event) / model + 1e-06)
        spread_rows(scale_ref, norm, 0)

    def glu_and_halo(layer, half):
        gated(layer, half)
        if half == half_order[0]:
            for s in range(strips):
                halo_out[layer, :, strip(s)] = padded[s, rows : rows + HALO_ROWS, :].astype(
                    jnp.bfloat16
                )

            @pl.when(has_next)
            def _():
                halo_copy(layer).start()

    def emit_f(layer, half):
        if half == 0:

            @pl.when(has_prev)
            def _():
                halo_copy(layer).wait_recv()
                for s in range(strips):
                    padded[s, 0:HALO_ROWS, :] = halo_in[layer, :, strip(s)].astype(jnp.float32)

            @pl.when(spot == 0)
            def _():
                padded[:, 0:HALO_ROWS, :] = jnp.zeros((strips, HALO_ROWS, LANES), jnp.float32)

        filter_rows(layer, half)
        if half == 0:
            event = 4 * layer + 1
            pack_rows(event, 0, row_a)
            pack_rows(event, groups, row_b)
            send_stats(event)
        send_own(2 * layer + 1, half)

    first_out = 2 * pieces
    second = 3 * pieces
    midway = 5 * pieces + 1
    turns_of = (
        range(second - 1, second + pieces - 1),
        range(second + pieces - 1, 5 * pieces),
        range(5 * pieces, 6 * pieces),
    )

    def first_projections():
        crossings = [(z, half) for half in half_order]
        crossings += [(arrival(index), half) for index, half in relays]
        paced = list(range(first_out, second))
        kept = paced[3:]
        paced = paced[:3]

        def pace():
            if paced:
                ring_copy(paced.pop(0), 0, x_way).start()

        pace()
        pace()

        def after(index, half):
            pace()
            if (index, half) != relays[0]:
                cross(*crossings.pop(0))

        interleave(0, (), (), 0, after)
        for half in half_order:
            side_wait(0, z, half)
            for index in range(chips - 1):
                side_wait(0, arrival(index), half)
        row_scale(0)
        for load in loads[4:]:
            load.wait()
        for each in range(layers):
            for tap in range(tap_count):
                tap_rows[each, tap : tap + 1, :] = taps_ref[tap, each : each + 1, :]
        for which in range(2):
            for chunk in range(which * pieces, (which + 1) * pieces):
                finish_sub(chunk)
            for half in half_order:
                if which == 0:
                    while crossings and crossings[0][1] == half or len(crossings) > 1:
                        cross(*crossings.pop(0))
                    for index in range(-1, chips - 1):
                        cross_wait(z if index < 0 else arrival(index), half)
                project_other(which, half)
            for half in half_order:
                project_mine(which, half)
        for chunk in range(first_out, first_out + pieces // 2):
            turn_chunk(chunk, 0)
        turned = list(range(first_out + pieces // 2, second - 1))
        for half in half_order:
            for which in range(2):
                half_copy(which, half).wait_recv()
            glu_and_halo(0, half)
            if half == half_order[0]:
                for chunk in paced + kept:
                    ring_copy(chunk, 0, x_way).start()
            emit_f(0, half)
            if half == half_order[0]:
                for chunk in turned:
                    turn_chunk(chunk, midway - 1)
    def later_projections(layer):
        base = 3 * layer * pieces

        def chip_of(index):
            return z if index < 0 else arrival(index)

        def take(which, index, half):
            project_chip(layer, which, chip_of(index), half, index < 0)

        def after(index, half):
            if half == half_order[-1] and 0 < index < chips - 2:
                if index == 1:
                    for chunk in range(base, base + pieces):
                        finish_chunk(chunk)
                for done in [-1, 0, 1] if index == 1 else [index]:
                    for each in half_order:
                        side_wait(2 * layer, chip_of(done), each)
                        take(0, done, each)
        interleave(2 * layer, LATE_TURNS, turns_of[1], midway - 1, after)
        for half in half_order:
            side_wait(2 * layer, chip_of(chips - 2), half)
            take(0, chips - 2, half)
        row_scale(4 * layer)
        for chunk in range(base + pieces, base + 2 * pieces - 1):
            finish_chunk(chunk)
            project_chunk(layer, 1, chunk, slice(0, rows))
        finish_chunk(base + 2 * pieces - 1)
        for half in half_order:
            start, size = bounds(2 * layer, half)
            project_chunk(layer, 1, base + 2 * pieces - 1, slice(start, start + size))
            glu_and_halo(layer, half)
            if half == half_order[0]:
                start_until(midway + AHEAD - 1)
            emit_f(layer, half)

    def squares(start, tile):
        at_rows = pl.ds(start, tile)
        total = jnp.zeros((tile, LANES), jnp.float32)
        for s in range(strips):
            own = acc[0, at_rows, strip(s)].astype(jnp.bfloat16).astype(jnp.float32)
            total = total + own * own
        row_b[at_rows, :] = total

    for layer in range(layers):
        q = 2 * layer
        event = 4 * layer
        base = 3 * layer * pieces
        if layer == 0:
            first_projections()
        else:
            later_projections(layer)

        def normal(layer=layer, event=event):
            totals = total_stats(event + 1) / model
            centre = totals[0:groups, :]
            spread = jnp.maximum(totals[groups : 2 * groups, :] - centre * centre, 0.0)
            inverse = lax.rsqrt(spread + 1e-05)
            spread_rows(scale_ref, inverse, 0)
            spread_rows(shift_ref, centre * inverse, 0)
            if layer == 0:
                for step in range(1, count):
                    param_copy(step).wait_recv()
            for half in half_order:
                side_wait(2 * layer + 1, z, half)
                mix(layer, z, half)

        def ready(index, half, layer=layer, normal=normal):
            q = 2 * layer + 1
            if index == 0 and half == half_order[0]:
                return
            if index == 0:
                normal()
                for again in half_order:
                    side_wait(q, arrival(0), again)
                    mix(layer, arrival(0), again)
                return
            if index == chips - 2 and half == half_order[0]:
                for chunk in range((3 * layer + 2) * pieces, (3 * layer + 3) * pieces):
                    finish_chunk(chunk)
                for each in half_order:
                    for done in range(-1, chips - 2):
                        merge(layer, z if done < 0 else arrival(done), each, done < 0)
            side_wait(q, arrival(index), half)
            mix(layer, arrival(index), half)
            if index == chips - 2:
                merge(layer, arrival(index), half, False)
                tiles(q, half, squares)
                pack_rows(4 * layer + 3 - half, 0, row_b, *groups_of(q, half))
                send_stats(4 * layer + 3 - half)

        interleave(
            q + 1,
            LAST_TURNS if layer else OUT_TURNS,
            turns_of[2] if layer else turns_of[0],
            chunk_total if layer else midway - 1,
            ready,
        )
        def updated(at_rows, layer=layer):
            branch = acc[0, at_rows, :].astype(jnp.bfloat16).astype(jnp.float32)
            scale = jnp.concatenate([scale_ref[at_rows, :]] * strips, axis=1)
            before = (tok_ref if layer == 0 else stream)[at_rows, :].astype(jnp.float32)
            after = before + branch * scale * post_ref[layer : layer + 1, :]
            after = after.astype(jnp.bfloat16)
            if layer + 1 < layers:
                stream[at_rows, :] = after
            else:
                last[at_rows, :] = after
            return after.astype(jnp.float32)

        for half in half_order:
            scale = lax.rsqrt(total_stats(event + 3 - half) / model + 1e-06)
            spread_rows(scale_ref, scale, 0, *groups_of(q + 1, half))
            if layer + 1 < layers:
                emit_u(layer + 1, half, updated)
                send_own(q + 2, half)
                if half == 0:
                    pack_rows(event + 4, 0, row_a)
                    send_stats(event + 4)
            else:
                tiles(q + 1, half, lambda start, tile: updated(pl.ds(start, tile)))
                result_copy(half).start()

    sent = 2 * ((group_turns - 1) * piece + piece // 2)
    await_bytes(w_all.at[0, 0 : 2 * pieces * sent, :], sub_send.at[0])
    for chunk in range(chunk_total - 2 * pieces):
        await_bytes(
            w_all.at[0, 0 : 2 * ((turns - 1) * piece + piece // 2), :], ring_send.at[chunk]
        )
    for which in range(2):
        for half in range(HALVES):
            half_copy(which, half).wait_send()
    for q in range(2 * layers):
        drain(q)
    await_bytes(stat_in, stat_send.at[0])
    await_bytes(params.at[0 : count - 1], par_send.at[0])

    @pl.when(has_next)
    def _():
        for layer in range(layers):
            halo_copy(layer).wait_send()

    for half in half_order:
        result_copy(half).wait()


def shards(
    tokens, pre_gain, w_value, w_gate, conv_taps, conv_bias, norm_gain, norm_bias, w_out, post_gain
):
    ring = lax.axis_size("sp")
    count = lax.axis_size("tp")
    chips = count // 2
    layers, depth, width = w_value.shape
    rows = tokens.shape[0]
    pieces = max(1, min(4, depth // 256))
    chunks = 3 * layers * pieces
    strips = width // LANES
    stat_rows = max(8, 2 * rows // LANES)
    param_rows = -(-2 * layers // 8) * 8
    hbm = pl.BlockSpec(memory_space=pl.ANY)
    dma = pltpu.SemaphoreType.DMA
    taps = jnp.transpose(conv_taps, (1, 0, 2))
    loaded = [tokens, pre_gain, taps, conv_bias, norm_gain, norm_bias, post_gain]
    scratch = [pltpu.VMEM(array.shape, array.dtype) for array in loaded]
    scratch += [dma((len(loaded),))]
    scratch += [pltpu.VMEM(conv_taps.shape, conv_taps.dtype)]
    scratch += [
        pltpu.VMEM((3 * layers, depth * ring, width), jnp.bfloat16),
        pltpu.VMEM((layers, count, rows, width), jnp.bfloat16),
        pltpu.VMEM((layers, count, rows, width), jnp.bfloat16),
        pltpu.VMEM((count, rows, width), jnp.bfloat16),
        pltpu.VMEM((2, rows, width), jnp.float32),
        pltpu.VMEM((strips, HALO_ROWS + rows, LANES), jnp.float32),
        pltpu.VMEM((rows, LANES), jnp.float32),
        pltpu.VMEM((rows, LANES), jnp.float32),
        pltpu.VMEM((rows, LANES), jnp.float32),
        pltpu.VMEM((rows, LANES), jnp.float32),
        pltpu.VMEM((rows, width), jnp.bfloat16),
        pltpu.VMEM((rows, width), jnp.bfloat16),
        dma((HALVES,)),
        pltpu.VMEM((layers, HALO_ROWS, width), jnp.bfloat16),
        pltpu.VMEM((layers, HALO_ROWS, width), jnp.bfloat16),
        pltpu.VMEM((4 * layers, stat_rows, LANES), jnp.float32),
        pltpu.VMEM((4 * layers, count - 1, stat_rows, LANES), jnp.float32),
        pltpu.VMEM((count, param_rows, width), jnp.float32),
        pltpu.VMEM((count, rows, width), jnp.bfloat16),
        pltpu.VMEM((2, rows, width), jnp.bfloat16),
        pltpu.VMEM((2, rows, width), jnp.bfloat16),
    ]
    scratch += [dma((2 * layers,))] * 2 + [dma((2 * layers, chips, HALVES))]
    scratch += [dma((2 * layers,)), dma((2 * layers, chips, HALVES))]
    scratch += [dma((chunks - 2 * pieces,)), dma((chunks - 2 * pieces, ring // 2))]
    scratch += [dma((1,)), dma((2, 2 * pieces, max(1, ring // 4)))]
    scratch += [dma((3 * layers,))]
    scratch += [dma((chips, HALVES))] * 4
    scratch += [dma((2, HALVES))] * 2
    scratch += [dma((1,)), dma((4 * layers, count - 1))]
    scratch += [dma((1,)), dma((count - 1,))]
    scratch += [dma((layers,))] * 2
    flops = 2 * rows * model_width(tokens, count) * width * 3 * layers
    return pl.pallas_call(
        functools.partial(module_kernel, ring, count),
        out_shape=jax.ShapeDtypeStruct(tokens.shape, tokens.dtype),
        in_specs=[hbm] * 10,
        out_specs=hbm,
        scratch_shapes=scratch,
        compiler_params=pltpu.CompilerParams(
            collective_id=0, has_side_effects=True, vmem_limit_bytes=63 * 2**20
        ),
        cost_estimate=pl.CostEstimate(flops=flops, bytes_accessed=flops // 512, transcendentals=0),
        name="modules",
    )(
        tokens,
        pre_gain,
        w_value,
        w_gate,
        w_out,
        taps,
        conv_bias,
        norm_gain,
        norm_bias,
        post_gain,
    )


def model_width(tokens, count):
    return tokens.shape[1] * count


def solution(mesh):
    in_specs = (
        P("sp", "tp"),
        P(),
        P(None, "sp", "tp"),
        P(None, "sp", "tp"),
        P(None, None, "tp"),
        P(None, "tp"),
        P(None, "tp"),
        P(None, "tp"),
        P(None, "sp", "tp"),
        P(None, "tp"),
    )
    out_specs = P("sp", "tp")
    return jax.shard_map(shards, mesh=mesh, in_specs=in_specs, out_specs=out_specs, check_vma=False)
```

```python
import functools

import jax
import jax.numpy as jnp
from jax import lax
from jax.experimental import pallas as pl
from jax.experimental.pallas import tpu as pltpu
from jax.sharding import PartitionSpec as P

MESH = pl.DeviceIdType.MESH
LANES = 128
HALVES = 2
AHEAD = 3
TILE_MOST = 112
HALO_ROWS = 32
LATE_TURNS = (0, 1, 3, 5)
OUT_TURNS = (2, 3, 4)
LAST_TURNS = (0, 1, 2, 4)


def gray_of(position, count):
    bits = [(position // 2**k) % 2 for k in range(count.bit_length())]
    return sum(((bits[k] + bits[k + 1]) % 2) * 2**k for k in range(count.bit_length() - 1))


def position_of(index, count):
    bits = [(index // 2**k) % 2 for k in range(count.bit_length() - 1)]
    return sum((sum(bits[k:]) % 2) * 2**k for k in range(count.bit_length() - 1))


def loop(count, body):
    def step(index, carry):
        body(index)
        return carry

    lax.fori_loop(0, count, step, 0)


def remote(src, dst, send_sem, recv_sem, axis, target):
    return pltpu.make_async_remote_copy(
        src_ref=src,
        dst_ref=dst,
        send_sem=send_sem,
        recv_sem=recv_sem,
        device_id={axis: target},
        device_id_type=MESH,
    )


def module_kernel(
    ring,
    count,
    tok_hbm,
    pre_hbm,
    value_ref,
    gate_ref,
    wout_ref,
    taps_hbm,
    bias_hbm,
    ngain_hbm,
    nbias_hbm,
    post_hbm,
    last,
    stream,
    final,
    gain_ref,
    tok_ref,
    pre_ref,
    taps_ref,
    bias_ref,
    ngain_ref,
    nbias_ref,
    post_ref,
    load_sem,
    tap_rows,
    w_all,
    u_all,
    f_all,
    mixed,
    acc,
    padded,
    row_a,
    row_b,
    scale_ref,
    shift_ref,
    halo_out,
    halo_in,
    stat_out,
    stat_in,
    params,
    x_all,
    half_out,
    half_in,
    z_up,
    z_down,
    z_recv,
    side_send,
    side_recv,
    ring_send,
    ring_recv,
    sub_send,
    sub_recv,
    own_sem,
    x_send,
    x_recv,
    pass_send,
    pass_recv,
    half_send,
    half_recv,
    stat_send,
    stat_recv,
    par_send,
    par_recv,
    halo_send,
    halo_recv,
):
    layers, depth, width = value_ref.shape
    rows = tok_ref.shape[0]
    model = width * count
    tap_count = taps_ref.shape[0]
    chips = count // 2
    strips = width // LANES
    groups = rows // LANES
    half_order = tuple(reversed(range(HALVES)))
    pieces = max(1, min(4, depth // 256))
    piece = depth // pieces
    turns = ring // 2
    group = ring // 2
    group_turns = max(1, group // 2)
    blocks_held = depth // width

    def bounds(q, half):
        split = rows // 2 - HALO_ROWS * (layers - (q + 1) // 2)
        return (split, rows - split) if half else (0, split)

    def rows_of(q, half):
        start, size = bounds(q, half)
        return pl.ds(start, size)

    def groups_of(q, half):
        start, size = bounds(q, half)
        return start // LANES, -(-(start + size) // LANES)

    def tiles(q, half, body):
        start, size = bounds(q, half)
        tile = max(t for t in range(16, TILE_MOST + 1, 16) if size % t == 0)
        loop(size // tile, lambda index: body(pl.multiple_of(start + index * tile, 16), tile))

    me = lax.axis_index("tp")
    z = me // 2
    core = me - 2 * z
    partner = me + 1 - 2 * core
    has_up = z < chips - 1
    has_down = z > 0
    spot = lax.axis_index("sp")
    at = position_of(spot, ring)
    ahead = gray_of((at + 1) % ring, ring)
    behind = gray_of((at + ring - 1) % ring, ring)
    low_bit = spot % 2
    pair = spot + 1 - 2 * low_bit
    group_at = position_of(spot // 2, group)
    group_ahead = 2 * gray_of((group_at + 1) % group, group) + low_bit
    group_behind = 2 * gray_of((group_at + group - 1) % group, group) + low_bit
    x_way = at % 2
    has_next = spot < ring - 1
    has_prev = spot > 0

    barrier = pltpu.get_barrier_semaphore()
    for step in range(1, count):
        pl.semaphore_signal(
            barrier, inc=1, device_id={"tp": lax.rem(me + step, count)}, device_id_type=MESH
        )
    pl.semaphore_signal(barrier, inc=1, device_id={"sp": ahead}, device_id_type=MESH)
    pl.semaphore_signal(barrier, inc=1, device_id={"sp": behind}, device_id_type=MESH)
    if group > 2:
        for member in (group_ahead, group_behind):
            pl.semaphore_signal(barrier, inc=1, device_id={"sp": member}, device_id_type=MESH)

    @pl.when(has_next)
    def _():
        pl.semaphore_signal(barrier, inc=1, device_id={"sp": spot + 1}, device_id_type=MESH)

    @pl.when(has_prev)
    def _():
        pl.semaphore_signal(barrier, inc=1, device_id={"sp": spot - 1}, device_id_type=MESH)

    loads = [
        pltpu.make_async_copy(source, there, load_sem.at[number])
        for number, (source, there) in enumerate(
            [
                (tok_hbm, tok_ref),
                (pre_hbm, pre_ref),
                (ngain_hbm, ngain_ref),
                (nbias_hbm, nbias_ref),
                (taps_hbm, taps_ref),
                (bias_hbm, bias_ref),
                (post_hbm, post_ref),
            ]
        )
    ]
    for load in loads:
        load.start()

    pl.semaphore_wait(
        barrier,
        count + (3 if group > 2 else 1) + has_next.astype(jnp.int32) + has_prev.astype(jnp.int32)
    )

    sources = (value_ref, gate_ref, wout_ref)
    chunk_total = 3 * layers * pieces

    def held(chunk, owner, first, size):
        start = owner * depth + (chunk % pieces) * piece + first
        return w_all.at[chunk // pieces, pl.ds(pl.multiple_of(start, size), size), :]

    def own_rows(chunk, first, size):
        projection = chunk // pieces
        return sources[projection % 3].at[
            projection // 3, pl.ds((chunk % pieces) * piece + first, size), :
        ]

    def ring_copy(chunk, step, way):
        owner = gray_of((at + ring - (1 - 2 * way) * step) % ring, ring)
        last = step == turns - 1
        size = piece // 2 if last else piece
        there = held(chunk, owner, size * way if last else 0, size)
        return remote(
            own_rows(chunk, 0, size) if step == 0 else there,
            there,
            ring_send.at[chunk - 2 * pieces],
            ring_recv.at[chunk - 2 * pieces, step],
            "sp",
            ahead * (1 - way) + behind * way,
        )

    def sub_copy(chunk, step, way):
        owner = 2 * gray_of((group_at + group - (1 - 2 * way) * step) % group, group) + low_bit
        last = step == group_turns - 1
        size = piece // 2 if last else piece
        first = size * way if last else 0
        there = held(chunk, owner, first, size)
        return remote(
            own_rows(chunk, first, size) if step == 0 else there,
            there,
            sub_send.at[0],
            sub_recv.at[way, chunk, step],
            "sp",
            group_behind if way else group_ahead,
        )

    def finish_sub(chunk):
        for step in range(group_turns - 1):
            for way in range(2):
                sub_copy(chunk, step, way).wait_recv()
                sub_copy(chunk, step + 1, way).start()
        for way in range(2):
            sub_copy(chunk, group_turns - 1, way).wait_recv()
        if chunk % pieces == 0:
            own_copy(chunk // pieces).wait()

    def own_copy(projection):
        return pltpu.make_async_copy(
            sources[projection % 3].at[projection // 3],
            w_all.at[projection, pl.ds(pl.multiple_of(spot * depth, depth), depth), :],
            own_sem.at[projection],
        )

    def await_bytes(ref, sem):
        pltpu.make_async_copy(ref, ref, sem).wait()

    def ring_arrived(chunk, step):
        size = 2 * piece if step < turns - 1 else piece
        await_bytes(w_all.at[0, 0:size, :], ring_recv.at[chunk - 2 * pieces, step])

    def whole_turn(chunk):
        owner = gray_of((at + ring - (2 * x_way - 1)) % ring, ring)
        there = held(chunk, owner, 0, piece)
        return remote(
            there,
            there,
            ring_send.at[chunk - 2 * pieces],
            ring_recv.at[chunk - 2 * pieces, turns - 1],
            "sp",
            ahead * x_way + behind * (1 - x_way),
        )

    second = 3 * pieces
    started = [3 * pieces]

    def start_until(last):
        while started[0] <= min(last, chunk_total - 1):
            for way in range(2):
                ring_copy(started[0], 0, way).start()
            started[0] += 1

    def turn_chunk(chunk, most):
        for step in range(turns - 1):
            ring_arrived(chunk, step)
            if ring == 4 and chunk == second:
                whole_turn(chunk).start()
            else:
                for way in range(2):
                    ring_copy(chunk, step + 1, way).start()
        if chunk < 5 * pieces - 1:
            most = min(most, 5 * pieces - 1)
        start_until(min(chunk + AHEAD, most))

    def finish_chunk(chunk):
        ring_arrived(chunk, turns - 1)
        if chunk % pieces == 0:
            own_copy(chunk // pieces).wait()

    def stage(q):
        return (u_all if q % 2 == 0 else f_all).at[q // 2]

    def part(q, block, half):
        return stage(q).at[block, rows_of(q, half), :]

    def up(q, chip, half):
        there = part(q, 2 * chip + core, half)
        return remote(
            there, there, z_up.at[q], z_recv.at[q, chip, half], "tp", me + 2
        )

    def down(q, chip, half):
        there = part(q, 2 * chip + core, half)
        return remote(
            there, there, z_down.at[q], z_recv.at[q, chip, half], "tp", me - 2
        )

    def side(q, chip, half):
        there = part(q, 2 * chip + core, half)
        return remote(
            there, there, side_send.at[q], side_recv.at[q, chip, half], "tp", partner
        )

    def side_wait(q, chip, half):
        there = part(q, 2 * chip + 1 - core, half)
        remote(
            there, there, side_send.at[q], side_recv.at[q, chip, half], "tp", partner
        ).wait_recv()

    def mine(block):
        return (block // blocks_held) % 2 == low_bit

    def x_copy(chip, half):
        block = 2 * chip + core
        return remote(
            part(0, block, half),
            x_all.at[block, rows_of(0, half), :],
            x_send.at[chip, half],
            x_recv.at[chip, half],
            "sp",
            pair,
        )

    def pass_copy(chip, half, block):
        there = x_all.at[block, rows_of(0, half), :]
        return remote(
            there, there, pass_send.at[chip, half], pass_recv.at[chip, half], "tp", partner
        )

    def cross(chip, half):
        @pl.when(mine(2 * chip + core))
        def _():
            x_copy(chip, half).wait_recv()
            pass_copy(chip, half, 2 * chip + core).start()

    def cross_wait(chip, half):
        @pl.when(mine(2 * chip + 1 - core))
        def _():
            pass_copy(chip, half, 2 * chip + 1 - core).wait_recv()

    def half_copy(which, half):
        at_rows = rows_of(0, half)
        return remote(
            half_out.at[which, at_rows, :],
            half_in.at[which, at_rows, :],
            half_send.at[which, half],
            half_recv.at[which, half],
            "sp",
            pair,
        )

    def send_own(q, half):
        if q == 0:

            @pl.when(jnp.logical_not(mine(me)))
            def _():
                x_copy(z, half).start()

        @pl.when(has_up)
        def _():
            up(q, z, half).start()

        @pl.when(has_down)
        def _():
            down(q, z, half).start()

        side(q, z, half).start()

    low = z + (2 * z > chips - 1).astype(jnp.int32) * (chips - 1 - 2 * z)
    upward = 1 - 2 * (2 * z > chips - 1).astype(jnp.int32)

    def arrival(index):
        both = (index < 2 * low).astype(jnp.int32)
        paired = z + (index // 2 + 1) * (1 if index % 2 else -1)
        alone = z + (index - low + 1) * upward
        return both * paired + (1 - both) * alone

    def relay(q, index, half):
        for sign in (-1, 1):
            chip = z + sign * (index + 1)

            @pl.when((chip >= 0) & (chip < chips))
            def _():
                there = part(q, 2 * chip + core, half)
                remote(
                    there, there, z_up.at[q], z_recv.at[q, chip, half], "tp", partner
                ).wait_recv()

                if sign < 0:

                    @pl.when(has_up)
                    def _():
                        up(q, chip, half).start()

                else:

                    @pl.when(has_down)
                    def _():
                        down(q, chip, half).start()

                side(q, chip, half).start()
                if q == 0:

                    @pl.when(jnp.logical_not(mine(2 * chip + core)))
                    def _():
                        x_copy(chip, half).start()

    def drain(q):
        await_bytes(stage(q).at[0:chips], side_send.at[q])
        for chip in range(chips):

            @pl.when(has_up & (z == chip))
            def _():
                await_bytes(stage(q).at[0 : chip + 1], z_up.at[q])

            @pl.when(has_down & (z == chip))
            def _():
                await_bytes(stage(q).at[0 : chips - chip], z_down.at[q])

        if q == 0:
            for chip in range(chips):
                for half in range(HALVES):

                    @pl.when(mine(2 * chip + core))
                    def _():
                        pass_copy(chip, half, 2 * chip + core).wait_send()

                    @pl.when(jnp.logical_not(mine(2 * chip + core)))
                    def _():
                        x_copy(chip, half).wait_send()

    def stat_copy(event, step):
        return remote(
            stat_out.at[event],
            stat_in.at[event, step - 1],
            stat_send.at[0],
            stat_recv.at[event],
            "tp",
            lax.rem(me + step, count),
        )

    def pack_rows(event, base, ref, first=0, last=groups):
        for group in range(first, last):
            turned = ref[group * LANES : (group + 1) * LANES, :].T
            stat_out[event, base + group : base + group + 1, :] = jnp.sum(
                turned, axis=0, keepdims=True
            )

    def send_stats(event):
        for step in range(1, count):
            stat_copy(event, step).start()

    def total_stats(event):
        total = stat_out[event]
        await_bytes(stat_in.at[event], stat_recv.at[event])
        for step in range(1, count):
            total = total + stat_in[event, step - 1]
        return total

    def spread_rows(ref, packed, base, first=0, last=groups):
        for group in range(first, last):
            line = packed[base + group : base + group + 1, :]
            ref[group * LANES : (group + 1) * LANES, :] = jnp.broadcast_to(
                line, (LANES, LANES)
            ).T

    def strip(index):
        return slice(index * LANES, (index + 1) * LANES)

    def emit_u(layer, half, source):
        def body(start, tile):
            at_rows = pl.ds(start, tile)
            values = source(at_rows)
            squares = jnp.zeros((tile, LANES), jnp.float32)
            for s in range(strips):
                own = values[:, strip(s)]
                squares = squares + own * own
            row_a[at_rows, :] = squares
            gain = pre_ref[layer : layer + 1, pl.ds(pl.multiple_of(me * width, width), width)]
            u_all[layer, me, at_rows, :] = (values * gain).astype(jnp.bfloat16)

        tiles(2 * layer, half, body)

    column_tile = min(256, width)

    def columns(index):
        return pl.ds(pl.multiple_of(index * column_tile, column_tile), column_tile)

    def weigh(projection, block, index):
        at_block = pl.ds(pl.multiple_of(block * width, width), width)
        return w_all[projection, at_block, columns(index)]

    def project_part(which, half, source, keep):
        at_rows = rows_of(0, half)

        def body(index):
            total = None
            for member in range(group):
                for inner in range(blocks_held):
                    block = (2 * member + low_bit) * blocks_held + inner
                    product = jnp.dot(
                        source[block, at_rows, :],
                        weigh(which, block, index),
                        preferred_element_type=jnp.float32,
                    )
                    total = product if total is None else total + product
            keep(at_rows, columns(index), total)

        loop(width // column_tile, body)

    def project_other(which, half):
        def keep(at_rows, at_columns, total):
            half_out[which, at_rows, at_columns] = total.astype(jnp.bfloat16)

        project_part(which, half, x_all, keep)
        half_copy(which, half).start()

    def project_mine(which, half):
        def keep(at_rows, at_columns, total):
            acc[which, at_rows, at_columns] = total

        project_part(which, half, u_all.at[0], keep)

    def project_chip(layer, which, chip, half, first):
        at_rows = rows_of(2 * layer, half)

        def body(index):
            total = None
            for c in range(2):
                product = jnp.dot(
                    u_all[layer, 2 * chip + c, at_rows, :],
                    weigh(3 * layer + which, 2 * chip + c, index),
                    preferred_element_type=jnp.float32,
                )
                total = product if total is None else total + product
            if first:
                acc[which, at_rows, columns(index)] = total
            else:
                acc[which, at_rows, columns(index)] += total

        loop(width // column_tile, body)

    def project_chunk(layer, which, chunk, at_rows):
        offset = (chunk % pieces) * piece

        def body(index):
            total = None
            for owner in range(ring):
                first = owner * depth + offset
                product = jnp.dot(
                    u_all[layer, first // width, at_rows, first % width : first % width + piece],
                    w_all[3 * layer + which, first : first + piece, columns(index)],
                    preferred_element_type=jnp.float32,
                )
                total = product if total is None else total + product
            if chunk % pieces == 0:
                acc[which, at_rows, columns(index)] = total
            else:
                acc[which, at_rows, columns(index)] += total

        loop(width // column_tile, body)

    def gated(layer, half):
        def body(start, tile):
            at_rows = pl.ds(start, tile)
            scale = scale_ref[at_rows, :]
            for s in range(strips):
                value = acc[0, at_rows, strip(s)]
                gate = acc[1, at_rows, strip(s)]
                if layer == 0:
                    value = value + half_in[0, at_rows, strip(s)].astype(jnp.float32)
                    gate = gate + half_in[1, at_rows, strip(s)].astype(jnp.float32)
                value = value * scale
                gate = gate * scale
                glu = (value * (0.5 * (1.0 + jnp.tanh(0.5 * gate)))).astype(jnp.bfloat16)
                padded[s, pl.ds(pl.multiple_of(HALO_ROWS + start, 8), tile), :] = glu.astype(
                    jnp.float32
                )

        tiles(2 * layer, half, body)

    def filter_rows(layer, half):
        def body(start, tile):
            at_rows = pl.ds(start, tile)
            oldest = start + HALO_ROWS - (tap_count - 1)
            first = jnp.zeros((tile, LANES), jnp.float32)
            second = jnp.zeros((tile, LANES), jnp.float32)
            for s in range(strips):
                total = jnp.zeros((tile, LANES), jnp.float32) + bias_ref[
                    layer : layer + 1, strip(s)
                ]
                for tap in range(tap_count):
                    total = (
                        total
                        + padded[s, pl.ds(oldest + tap, tile), :]
                        * tap_rows[layer, tap : tap + 1, strip(s)]
                    )
                f_all[layer, me, at_rows, strip(s)] = total.astype(jnp.bfloat16)
                first = first + total
                second = second + total * total
            row_a[at_rows, :] = first
            row_b[at_rows, :] = second

        tiles(2 * layer + 1, half, body)

    def mix(layer, chip, half):
        for c in range(2):
            block = 2 * chip + c
            gains = params[block, 2 * layer : 2 * layer + 1, :]
            biases = params[block, 2 * layer + 1 : 2 * layer + 2, :]

            def body(start, tile):
                at_rows = pl.ds(start, tile)
                scale = scale_ref[at_rows, :]
                shift = shift_ref[at_rows, :]
                for s in range(strips):
                    shaped = f_all[layer, block, at_rows, strip(s)].astype(jnp.float32) * scale
                    shaped = (shaped - shift) * gains[:, strip(s)] + biases[:, strip(s)]
                    mixed[block, at_rows, strip(s)] = (
                        shaped * (0.5 * (1.0 + jnp.tanh(0.5 * shaped)))
                    ).astype(jnp.bfloat16)

            tiles(2 * layer + 1, half, body)

    def merge(layer, chip, half, first):
        at_rows = rows_of(2 * layer + 1, half)

        def body(index):
            total = None
            for c in range(2):
                block = 2 * chip + c
                product = jnp.dot(
                    mixed[block, at_rows, :],
                    weigh(3 * layer + 2, block, index),
                    preferred_element_type=jnp.float32,
                )
                total = product if total is None else total + product
            if first:
                acc[0, at_rows, columns(index)] = total
            else:
                acc[0, at_rows, columns(index)] += total

        loop(width // column_tile, body)

    for chunk in range(2 * pieces):
        for way in range(2):
            sub_copy(chunk, 0, way).start()
    for load in loads[:4]:
        load.wait()

    def from_tokens(at_rows):
        return tok_ref[at_rows, :].astype(jnp.float32)

    for half in half_order:
        emit_u(0, half, from_tokens)
        if half == half_order[0]:
            for layer in range(layers):
                params[me, 2 * layer : 2 * layer + 1, :] = ngain_ref[layer : layer + 1, :]
                params[me, 2 * layer + 1 : 2 * layer + 2, :] = nbias_ref[layer : layer + 1, :]
        send_own(0, half)

    def param_copy(step):
        return remote(
            params.at[me],
            params.at[me],
            par_send.at[0],
            par_recv.at[0],
            "tp",
            lax.rem(me + step, count),
        )

    for chunk in range(2 * pieces, 3 * pieces):
        ring_copy(chunk, 0, 1 - x_way).start()
    for projection in range(3 * layers):
        own_copy(projection).start()
    pack_rows(0, 0, row_a)
    send_stats(0)
    for step in range(1, count):
        param_copy(step).start()

    def halo_copy(layer):
        return remote(
            halo_out.at[layer],
            halo_in.at[layer],
            halo_send.at[layer],
            halo_recv.at[layer],
            "sp",
            lax.rem(spot + 1, ring),
        )

    relays = [(index, half) for index in range(chips - 1) for half in half_order]

    def interleave(q, turns_at, chunks, most, after):
        chunks = list(chunks)
        for number, (index, half) in enumerate(relays):
            for _ in range(turns_at.count(number)):
                if chunks:
                    turn_chunk(chunks.pop(0), most)
            relay(q, index, half)
            after(index, half)
        for chunk in chunks:
            turn_chunk(chunk, most)

    def row_scale(event):
        norm = lax.rsqrt(total_stats(event) / model + 1e-06)
        spread_rows(scale_ref, norm, 0)

    def glu_and_halo(layer, half):
        gated(layer, half)
        if half == half_order[0]:
            for s in range(strips):
                halo_out[layer, :, strip(s)] = padded[s, rows : rows + HALO_ROWS, :].astype(
                    jnp.bfloat16
                )

            @pl.when(has_next)
            def _():
                halo_copy(layer).start()

    def emit_f(layer, half):
        if half == 0:

            @pl.when(has_prev)
            def _():
                halo_copy(layer).wait_recv()
                for s in range(strips):
                    padded[s, 0:HALO_ROWS, :] = halo_in[layer, :, strip(s)].astype(jnp.float32)

            @pl.when(spot == 0)
            def _():
                padded[:, 0:HALO_ROWS, :] = jnp.zeros((strips, HALO_ROWS, LANES), jnp.float32)

        filter_rows(layer, half)
        if half == 0:
            event = 4 * layer + 1
            pack_rows(event, 0, row_a)
            pack_rows(event, groups, row_b)
            send_stats(event)
        send_own(2 * layer + 1, half)

    first_out = 2 * pieces
    midway = 5 * pieces + 1
    turns_of = (
        range(second - 1, second + pieces - 1),
        range(second + pieces - 1, 5 * pieces),
        range(5 * pieces, 6 * pieces),
    )

    def first_projections():
        crossings = [(z, half) for half in half_order]
        crossings += [(arrival(index), half) for index, half in relays]
        paced = list(range(first_out, second))
        kept = paced[3:]
        paced = paced[:3]

        def pace():
            if paced:
                ring_copy(paced.pop(0), 0, x_way).start()

        pace()
        pace()

        def after(index, half):
            pace()
            if (index, half) != relays[0]:
                cross(*crossings.pop(0))

        interleave(0, (), (), 0, after)
        for half in half_order:
            side_wait(0, z, half)
            for index in range(chips - 1):
                side_wait(0, arrival(index), half)
        row_scale(0)
        for load in loads[4:]:
            load.wait()
        for each in range(layers):
            for tap in range(tap_count):
                tap_rows[each, tap : tap + 1, :] = taps_ref[tap, each : each + 1, :]
        for which in range(2):
            for chunk in range(which * pieces, (which + 1) * pieces):
                finish_sub(chunk)
            for half in half_order:
                if which == 0:
                    while crossings and crossings[0][1] == half or len(crossings) > 1:
                        cross(*crossings.pop(0))
                    for index in range(-1, chips - 1):
                        cross_wait(z if index < 0 else arrival(index), half)
                project_other(which, half)
            for half in half_order:
                project_mine(which, half)
        for chunk in range(first_out, first_out + pieces // 2):
            turn_chunk(chunk, 0)
        turned = list(range(first_out + pieces // 2, second - 1))
        for half in half_order:
            for which in range(2):
                half_copy(which, half).wait_recv()
            glu_and_halo(0, half)
            if half == half_order[0]:
                for chunk in paced + kept:
                    ring_copy(chunk, 0, x_way).start()
            emit_f(0, half)
            if half == half_order[0]:
                for chunk in turned:
                    turn_chunk(chunk, midway - 1)
    def later_projections(layer):
        base = 3 * layer * pieces

        def chip_of(index):
            return z if index < 0 else arrival(index)

        def take(which, index, half):
            project_chip(layer, which, chip_of(index), half, index < 0)

        def after(index, half):
            if half == half_order[-1] and 0 < index < chips - 2:
                if index == 1:
                    for chunk in range(base, base + pieces):
                        finish_chunk(chunk)
                for done in [-1, 0, 1] if index == 1 else [index]:
                    for each in half_order:
                        side_wait(2 * layer, chip_of(done), each)
                        take(0, done, each)
        interleave(2 * layer, LATE_TURNS, turns_of[1], midway - 1, after)
        for half in half_order:
            side_wait(2 * layer, chip_of(chips - 2), half)
            take(0, chips - 2, half)
        row_scale(4 * layer)
        for chunk in range(base + pieces, base + 2 * pieces - 1):
            finish_chunk(chunk)
            project_chunk(layer, 1, chunk, slice(0, rows))
        finish_chunk(base + 2 * pieces - 1)
        for half in half_order:
            start, size = bounds(2 * layer, half)
            project_chunk(layer, 1, base + 2 * pieces - 1, slice(start, start + size))
            glu_and_halo(layer, half)
            if half == half_order[0]:
                start_until(midway + AHEAD - 1)
            emit_f(layer, half)

    def merge_chunk(layer, chunk, first):
        offset = (chunk % pieces) * piece

        def body(index):
            total = None
            for each in range(-1, chips - 2):
                chip = z if each < 0 else arrival(each)
                for c in range(2):
                    if c % blocks_held != offset // width:
                        continue
                    block = 2 * chip + c
                    start = block * width + offset % width
                    product = jnp.dot(
                        mixed[block, :, offset % width : offset % width + piece],
                        w_all[
                            3 * layer + 2, pl.ds(pl.multiple_of(start, piece), piece), columns(index)
                        ],
                        preferred_element_type=jnp.float32,
                    )
                    total = product if total is None else total + product
            if first:
                acc[0, :, columns(index)] = total
            else:
                acc[0, :, columns(index)] += total

        loop(width // column_tile, body)

    def squares(layer, start, tile):
        at_rows = pl.ds(start, tile)
        total = jnp.zeros((tile, LANES), jnp.float32)
        for s in range(strips):
            branch = acc[0, at_rows, strip(s)].astype(jnp.bfloat16)
            if layer == layers - 1:
                last[at_rows, strip(s)] = branch
            own = branch.astype(jnp.float32)
            total = total + own * own
        row_b[at_rows, :] = total

    for layer in range(layers):
        q = 2 * layer
        event = 4 * layer
        base = 3 * layer * pieces
        if layer == 0:
            first_projections()
        else:
            later_projections(layer)

        def normal(layer=layer, event=event):
            totals = total_stats(event + 1) / model
            centre = totals[0:groups, :]
            spread = jnp.maximum(totals[groups : 2 * groups, :] - centre * centre, 0.0)
            inverse = lax.rsqrt(spread + 1e-05)
            spread_rows(scale_ref, inverse, 0)
            spread_rows(shift_ref, centre * inverse, 0)
            if layer == 0:
                await_bytes(params.at[0 : count - 1], par_recv.at[0])
            for half in half_order:
                side_wait(2 * layer + 1, z, half)
                mix(layer, z, half)

        def ready(index, half, layer=layer, normal=normal):
            q = 2 * layer + 1
            if index == 0 and half == half_order[0]:
                return
            if index == 0:
                normal()
                for again in half_order:
                    side_wait(q, arrival(0), again)
                    mix(layer, arrival(0), again)
                return
            if index == chips - 2 and half == half_order[0]:
                for chunk in range((3 * layer + 2) * pieces, (3 * layer + 3) * pieces):
                    finish_chunk(chunk)
                    merge_chunk(layer, chunk, chunk % pieces == 0)
            side_wait(q, arrival(index), half)
            mix(layer, arrival(index), half)
            if index == chips - 2:
                merge(layer, arrival(index), half, False)
                tiles(q, half, functools.partial(squares, layer))
                pack_rows(4 * layer + 3 - half, 0, row_b, *groups_of(q, half))
                send_stats(4 * layer + 3 - half)

        interleave(
            q + 1,
            LAST_TURNS if layer else OUT_TURNS,
            turns_of[2] if layer else turns_of[0],
            chunk_total if layer else midway - 1,
            ready,
        )
        def updated(at_rows, layer=layer):
            branch = acc[0, at_rows, :].astype(jnp.bfloat16).astype(jnp.float32)
            scale = jnp.concatenate([scale_ref[at_rows, :]] * strips, axis=1)
            before = (tok_ref if layer == 0 else stream)[at_rows, :].astype(jnp.float32)
            after = before + branch * scale * post_ref[layer : layer + 1, :]
            after = after.astype(jnp.bfloat16)
            stream[at_rows, :] = after
            return after.astype(jnp.float32)

        for half in half_order:
            totals = total_stats(event + 3 - half)
            if layer + 1 < layers:
                scale = lax.rsqrt(totals / model + 1e-06)
                spread_rows(scale_ref, scale, 0, *groups_of(q + 1, half))
                emit_u(layer + 1, half, updated)
                send_own(q + 2, half)
                if half == 0:
                    pack_rows(event + 4, 0, row_a)
                    send_stats(event + 4)
            else:
                first, end = groups_of(q + 1, half)
                final[first:end, :] = totals[first:end, :]

    gain_ref[...] = post_ref[layers - 1 : layers, :]
    if layers == 1:
        stream[...] = tok_ref[...]
    sent = 2 * ((group_turns - 1) * piece + piece // 2)
    await_bytes(w_all.at[0, 0 : 2 * pieces * sent, :], sub_send.at[0])
    for chunk in range(chunk_total - 2 * pieces):
        await_bytes(
            w_all.at[0, 0 : 2 * ((turns - 1) * piece + piece // 2), :], ring_send.at[chunk]
        )
    for which in range(2):
        for half in range(HALVES):
            half_copy(which, half).wait_send()
    for q in range(2 * layers):
        drain(q)
    await_bytes(stat_in, stat_send.at[0])
    await_bytes(params.at[0 : count - 1], par_send.at[0])

    @pl.when(has_next)
    def _():
        for layer in range(layers):
            halo_copy(layer).wait_send()


def shards(
    tokens, pre_gain, w_value, w_gate, conv_taps, conv_bias, norm_gain, norm_bias, w_out, post_gain
):
    ring = lax.axis_size("sp")
    count = lax.axis_size("tp")
    chips = count // 2
    layers, depth, width = w_value.shape
    rows = tokens.shape[0]
    pieces = max(1, min(4, depth // 256))
    chunks = 3 * layers * pieces
    strips = width // LANES
    stat_rows = max(8, 2 * rows // LANES)
    param_rows = -(-2 * layers // 8) * 8
    hbm = pl.BlockSpec(memory_space=pl.ANY)
    dma = pltpu.SemaphoreType.DMA
    taps = jnp.transpose(conv_taps, (1, 0, 2))
    loaded = [tokens, pre_gain, taps, conv_bias, norm_gain, norm_bias, post_gain]
    scratch = [pltpu.VMEM(array.shape, array.dtype) for array in loaded]
    scratch += [dma((len(loaded),))]
    scratch += [pltpu.VMEM(conv_taps.shape, conv_taps.dtype)]
    scratch += [
        pltpu.VMEM((3 * layers, depth * ring, width), jnp.bfloat16),
        pltpu.VMEM((layers, count, rows, width), jnp.bfloat16),
        pltpu.VMEM((layers, count, rows, width), jnp.bfloat16),
        pltpu.VMEM((count, rows, width), jnp.bfloat16),
        pltpu.VMEM((2, rows, width), jnp.float32),
        pltpu.VMEM((strips, HALO_ROWS + rows, LANES), jnp.float32),
        pltpu.VMEM((rows, LANES), jnp.float32),
        pltpu.VMEM((rows, LANES), jnp.float32),
        pltpu.VMEM((rows, LANES), jnp.float32),
        pltpu.VMEM((rows, LANES), jnp.float32),
        pltpu.VMEM((layers, HALO_ROWS, width), jnp.bfloat16),
        pltpu.VMEM((layers, HALO_ROWS, width), jnp.bfloat16),
        pltpu.VMEM((4 * layers, stat_rows, LANES), jnp.float32),
        pltpu.VMEM((4 * layers, count - 1, stat_rows, LANES), jnp.float32),
        pltpu.VMEM((count, param_rows, width), jnp.float32),
        pltpu.VMEM((count, rows, width), jnp.bfloat16),
        pltpu.VMEM((2, rows, width), jnp.bfloat16),
        pltpu.VMEM((2, rows, width), jnp.bfloat16),
    ]
    scratch += [dma((2 * layers,))] * 2 + [dma((2 * layers, chips, HALVES))]
    scratch += [dma((2 * layers,)), dma((2 * layers, chips, HALVES))]
    scratch += [dma((chunks - 2 * pieces,)), dma((chunks - 2 * pieces, ring // 2))]
    scratch += [dma((1,)), dma((2, 2 * pieces, max(1, ring // 4)))]
    scratch += [dma((3 * layers,))]
    scratch += [dma((chips, HALVES))] * 4
    scratch += [dma((2, HALVES))] * 2
    scratch += [dma((1,)), dma((4 * layers,))]
    scratch += [dma((1,)), dma((1,))]
    scratch += [dma((layers,))] * 2
    flops = 2 * rows * model_width(tokens, count) * width * 3 * layers
    branch, before, totals, gain = pl.pallas_call(
        functools.partial(module_kernel, ring, count),
        out_shape=[
            pltpu.VMEM(tokens.shape, tokens.dtype),
            pltpu.VMEM(tokens.shape, tokens.dtype),
            pltpu.VMEM((stat_rows, LANES), jnp.float32),
            pltpu.VMEM((1, width), jnp.float32),
        ],
        in_specs=[hbm] * 10,
        out_specs=[pl.BlockSpec(memory_space=pltpu.VMEM)] * 4,
        scratch_shapes=scratch,
        compiler_params=pltpu.CompilerParams(
            collective_id=0, has_side_effects=True, vmem_limit_bytes=60 * 2**20
        ),
        cost_estimate=pl.CostEstimate(flops=flops, bytes_accessed=flops // 512, transcendentals=0),
        name="modules",
    )(
        tokens,
        pre_gain,
        w_value,
        w_gate,
        w_out,
        taps,
        conv_bias,
        norm_gain,
        norm_bias,
        post_gain,
    )
    total = totals[: rows // LANES].reshape(rows)
    rescale = lax.rsqrt(total / model_width(tokens, count) + 1e-06)[:, None]
    after = before.astype(jnp.float32) + branch.astype(jnp.float32) * rescale * gain
    return after.astype(jnp.bfloat16)


def model_width(tokens, count):
    return tokens.shape[1] * count


def solution(mesh):
    in_specs = (
        P("sp", "tp"),
        P(),
        P(None, "sp", "tp"),
        P(None, "sp", "tp"),
        P(None, None, "tp"),
        P(None, "tp"),
        P(None, "tp"),
        P(None, "tp"),
        P(None, "sp", "tp"),
        P(None, "tp"),
    )
    out_specs = P("sp", "tp")
    return jax.shard_map(shards, mesh=mesh, in_specs=in_specs, out_specs=out_specs, check_vma=False)
```

```python
import functools

import jax
import jax.numpy as jnp
from jax import lax
from jax.experimental import pallas as pl
from jax.experimental.pallas import tpu as pltpu
from jax.sharding import PartitionSpec as P

MESH = pl.DeviceIdType.MESH
LANES = 128
HALVES = 2
AHEAD = 3
TILE_MOST = 112
HALO_ROWS = 32
LATE_TURNS = (0, 1, 3, 5)
OUT_TURNS = (2, 3, 4)
LAST_TURNS = (0, 1, 2, 4)


def gray_of(position, count):
    bits = [(position // 2**k) % 2 for k in range(count.bit_length())]
    return sum(((bits[k] + bits[k + 1]) % 2) * 2**k for k in range(count.bit_length() - 1))


def position_of(index, count):
    bits = [(index // 2**k) % 2 for k in range(count.bit_length() - 1)]
    return sum((sum(bits[k:]) % 2) * 2**k for k in range(count.bit_length() - 1))


def loop(count, body):
    def step(index, carry):
        body(index)
        return carry

    lax.fori_loop(0, count, step, 0)


def remote(src, dst, send_sem, recv_sem, axis, target):
    return pltpu.make_async_remote_copy(
        src_ref=src,
        dst_ref=dst,
        send_sem=send_sem,
        recv_sem=recv_sem,
        device_id={axis: target},
        device_id_type=MESH,
    )


def module_kernel(
    ring,
    count,
    tok_hbm,
    pre_hbm,
    value_ref,
    gate_ref,
    wout_ref,
    taps_hbm,
    bias_hbm,
    ngain_hbm,
    nbias_hbm,
    post_hbm,
    last,
    stream,
    final,
    gain_ref,
    tok_ref,
    pre_ref,
    taps_ref,
    bias_ref,
    ngain_ref,
    nbias_ref,
    post_ref,
    load_sem,
    tap_rows,
    w_all,
    u_all,
    f_all,
    mixed,
    acc,
    padded,
    row_a,
    row_b,
    scale_ref,
    shift_ref,
    halo_out,
    halo_in,
    stat_out,
    stat_in,
    params,
    x_all,
    half_out,
    half_in,
    z_up,
    z_down,
    z_recv,
    side_send,
    side_recv,
    ring_send,
    ring_recv,
    sub_send,
    sub_recv,
    own_sem,
    x_send,
    x_recv,
    pass_send,
    pass_recv,
    half_send,
    half_recv,
    stat_send,
    stat_recv,
    par_send,
    par_recv,
    halo_send,
    halo_recv,
):
    layers, depth, width = value_ref.shape
    rows = tok_ref.shape[0]
    model = width * count
    tap_count = taps_ref.shape[0]
    chips = count // 2
    strips = width // LANES
    groups = rows // LANES
    half_order = tuple(reversed(range(HALVES)))
    pieces = max(1, min(4, depth // 256))
    piece = depth // pieces
    turns = ring // 2
    group = ring // 2
    group_turns = max(1, group // 2)
    blocks_held = depth // width

    def bounds(q, half):
        split = rows // 2 - HALO_ROWS * (layers - (q + 1) // 2)
        return (split, rows - split) if half else (0, split)

    def rows_of(q, half):
        start, size = bounds(q, half)
        return pl.ds(start, size)

    def groups_of(q, half):
        start, size = bounds(q, half)
        return start // LANES, -(-(start + size) // LANES)

    def tiles(q, half, body):
        start, size = bounds(q, half)
        tile = max(t for t in range(16, TILE_MOST + 1, 16) if size % t == 0)
        loop(size // tile, lambda index: body(pl.multiple_of(start + index * tile, 16), tile))

    me = lax.axis_index("tp")
    z = me // 2
    core = me - 2 * z
    partner = me + 1 - 2 * core
    has_up = z < chips - 1
    has_down = z > 0
    spot = lax.axis_index("sp")
    at = position_of(spot, ring)
    ahead = gray_of((at + 1) % ring, ring)
    behind = gray_of((at + ring - 1) % ring, ring)
    low_bit = spot % 2
    pair = spot + 1 - 2 * low_bit
    group_at = position_of(spot // 2, group)
    group_ahead = 2 * gray_of((group_at + 1) % group, group) + low_bit
    group_behind = 2 * gray_of((group_at + group - 1) % group, group) + low_bit
    x_way = at % 2
    has_next = spot < ring - 1
    has_prev = spot > 0

    barrier = pltpu.get_barrier_semaphore()
    for step in range(1, count):
        pl.semaphore_signal(
            barrier, inc=1, device_id={"tp": lax.rem(me + step, count)}, device_id_type=MESH
        )
    pl.semaphore_signal(barrier, inc=1, device_id={"sp": ahead}, device_id_type=MESH)
    pl.semaphore_signal(barrier, inc=1, device_id={"sp": behind}, device_id_type=MESH)
    if group > 2:
        for member in (group_ahead, group_behind):
            pl.semaphore_signal(barrier, inc=1, device_id={"sp": member}, device_id_type=MESH)

    @pl.when(has_next)
    def _():
        pl.semaphore_signal(barrier, inc=1, device_id={"sp": spot + 1}, device_id_type=MESH)

    @pl.when(has_prev)
    def _():
        pl.semaphore_signal(barrier, inc=1, device_id={"sp": spot - 1}, device_id_type=MESH)

    loads = [
        pltpu.make_async_copy(source, there, load_sem.at[number])
        for number, (source, there) in enumerate(
            [
                (tok_hbm, tok_ref),
                (pre_hbm, pre_ref),
                (ngain_hbm, ngain_ref),
                (nbias_hbm, nbias_ref),
                (taps_hbm, taps_ref),
                (bias_hbm, bias_ref),
                (post_hbm, post_ref),
            ]
        )
    ]
    for load in loads:
        load.start()

    sources = (value_ref, gate_ref, wout_ref)
    chunk_total = 3 * layers * pieces

    def held(chunk, owner, first, size):
        start = owner * depth + (chunk % pieces) * piece + first
        return w_all.at[chunk // pieces, pl.ds(pl.multiple_of(start, size), size), :]

    def own_rows(chunk, first, size):
        projection = chunk // pieces
        return sources[projection % 3].at[
            projection // 3, pl.ds((chunk % pieces) * piece + first, size), :
        ]

    def ring_copy(chunk, step, way):
        owner = gray_of((at + ring - (1 - 2 * way) * step) % ring, ring)
        last = step == turns - 1
        size = piece // 2 if last else piece
        there = held(chunk, owner, size * way if last else 0, size)
        return remote(
            own_rows(chunk, 0, size) if step == 0 else there,
            there,
            ring_send.at[chunk - 2 * pieces],
            ring_recv.at[chunk - 2 * pieces, step],
            "sp",
            ahead * (1 - way) + behind * way,
        )

    def sub_copy(chunk, step, way):
        owner = 2 * gray_of((group_at + group - (1 - 2 * way) * step) % group, group) + low_bit
        last = step == group_turns - 1
        size = piece // 2 if last else piece
        first = size * way if last else 0
        there = held(chunk, owner, first, size)
        return remote(
            own_rows(chunk, first, size) if step == 0 else there,
            there,
            sub_send.at[0],
            sub_recv.at[way, chunk, step],
            "sp",
            group_behind if way else group_ahead,
        )

    def finish_sub(chunk):
        for step in range(group_turns - 1):
            for way in range(2):
                sub_copy(chunk, step, way).wait_recv()
                sub_copy(chunk, step + 1, way).start()
        for way in range(2):
            sub_copy(chunk, group_turns - 1, way).wait_recv()
        if chunk % pieces == 0:
            own_copy(chunk // pieces).wait()

    def own_copy(projection):
        return pltpu.make_async_copy(
            sources[projection % 3].at[projection // 3],
            w_all.at[projection, pl.ds(pl.multiple_of(spot * depth, depth), depth), :],
            own_sem.at[projection],
        )

    def await_bytes(ref, sem):
        pltpu.make_async_copy(ref, ref, sem).wait()

    def ring_arrived(chunk, step):
        size = 2 * piece if step < turns - 1 else piece
        await_bytes(w_all.at[0, 0:size, :], ring_recv.at[chunk - 2 * pieces, step])

    def uneven_turn(chunk, way, first, size):
        owner = gray_of((at + ring - (1 - 2 * way)) % ring, ring)
        start = owner * depth + (chunk % pieces) * piece + first
        there = w_all.at[chunk // pieces, pl.ds(pl.multiple_of(start, piece // 4), size), :]
        return remote(
            there,
            there,
            ring_send.at[chunk - 2 * pieces],
            ring_recv.at[chunk - 2 * pieces, turns - 1],
            "sp",
            ahead * (1 - way) + behind * way,
        )

    second = 3 * pieces
    started = [3 * pieces]

    def start_until(last):
        while started[0] <= min(last, chunk_total - 1):
            for way in range(2):
                ring_copy(started[0], 0, way).start()
            started[0] += 1

    def turn_chunk(chunk, most):
        for step in range(turns - 1):
            ring_arrived(chunk, step)
            if ring == 4 and chunk == second:
                most_rows = 3 * (piece // 4)
                uneven_turn(chunk, 1 - x_way, 0, most_rows).start()
                uneven_turn(chunk, x_way, most_rows, piece - most_rows).start()
            else:
                for way in range(2):
                    ring_copy(chunk, step + 1, way).start()
        if chunk < 5 * pieces - 1:
            most = min(most, 5 * pieces - 1)
        start_until(min(chunk + AHEAD, most))

    def finish_chunk(chunk):
        ring_arrived(chunk, turns - 1)
        if chunk % pieces == 0:
            own_copy(chunk // pieces).wait()

    def stage(q):
        return (u_all if q % 2 == 0 else f_all).at[q // 2]

    def part(q, block, half):
        return stage(q).at[block, rows_of(q, half), :]

    def up(q, chip, half):
        there = part(q, 2 * chip + core, half)
        return remote(
            there, there, z_up.at[q], z_recv.at[q, chip, half], "tp", me + 2
        )

    def down(q, chip, half):
        there = part(q, 2 * chip + core, half)
        return remote(
            there, there, z_down.at[q], z_recv.at[q, chip, half], "tp", me - 2
        )

    def side(q, chip, half):
        there = part(q, 2 * chip + core, half)
        return remote(
            there, there, side_send.at[q], side_recv.at[q, chip, half], "tp", partner
        )

    def side_wait(q, chip, half):
        there = part(q, 2 * chip + 1 - core, half)
        remote(
            there, there, side_send.at[q], side_recv.at[q, chip, half], "tp", partner
        ).wait_recv()

    def mine(block):
        return (block // blocks_held) % 2 == low_bit

    def x_copy(chip, half):
        block = 2 * chip + core
        return remote(
            part(0, block, half),
            x_all.at[block, rows_of(0, half), :],
            x_send.at[chip, half],
            x_recv.at[chip, half],
            "sp",
            pair,
        )

    def pass_copy(chip, half, block):
        there = x_all.at[block, rows_of(0, half), :]
        return remote(
            there, there, pass_send.at[chip, half], pass_recv.at[chip, half], "tp", partner
        )

    def cross(chip, half):
        @pl.when(mine(2 * chip + core))
        def _():
            x_copy(chip, half).wait_recv()
            pass_copy(chip, half, 2 * chip + core).start()

    def cross_wait(chip, half):
        @pl.when(mine(2 * chip + 1 - core))
        def _():
            pass_copy(chip, half, 2 * chip + 1 - core).wait_recv()

    def half_copy(which, half):
        at_rows = rows_of(0, half)
        return remote(
            half_out.at[which, at_rows, :],
            half_in.at[which, at_rows, :],
            half_send.at[which, half],
            half_recv.at[which, half],
            "sp",
            pair,
        )

    def send_own(q, half):
        if q == 0:

            @pl.when(jnp.logical_not(mine(me)))
            def _():
                x_copy(z, half).start()

        @pl.when(has_up)
        def _():
            up(q, z, half).start()

        @pl.when(has_down)
        def _():
            down(q, z, half).start()

        side(q, z, half).start()

    low = z + (2 * z > chips - 1).astype(jnp.int32) * (chips - 1 - 2 * z)
    upward = 1 - 2 * (2 * z > chips - 1).astype(jnp.int32)

    def arrival(index):
        both = (index < 2 * low).astype(jnp.int32)
        paired = z + (index // 2 + 1) * (1 if index % 2 else -1)
        alone = z + (index - low + 1) * upward
        return both * paired + (1 - both) * alone

    def relay(q, index, half):
        for sign in (-1, 1):
            chip = z + sign * (index + 1)

            @pl.when((chip >= 0) & (chip < chips))
            def _():
                there = part(q, 2 * chip + core, half)
                remote(
                    there, there, z_up.at[q], z_recv.at[q, chip, half], "tp", partner
                ).wait_recv()

                if sign < 0:

                    @pl.when(has_up)
                    def _():
                        up(q, chip, half).start()

                else:

                    @pl.when(has_down)
                    def _():
                        down(q, chip, half).start()

                side(q, chip, half).start()
                if q == 0:

                    @pl.when(jnp.logical_not(mine(2 * chip + core)))
                    def _():
                        x_copy(chip, half).start()

    def drain(q):
        await_bytes(stage(q).at[0:chips], side_send.at[q])
        for chip in range(chips):

            @pl.when(has_up & (z == chip))
            def _():
                await_bytes(stage(q).at[0 : chip + 1], z_up.at[q])

            @pl.when(has_down & (z == chip))
            def _():
                await_bytes(stage(q).at[0 : chips - chip], z_down.at[q])

        if q == 0:
            for chip in range(chips):
                for half in range(HALVES):

                    @pl.when(mine(2 * chip + core))
                    def _():
                        pass_copy(chip, half, 2 * chip + core).wait_send()

                    @pl.when(jnp.logical_not(mine(2 * chip + core)))
                    def _():
                        x_copy(chip, half).wait_send()

    def stat_copy(event, step):
        return remote(
            stat_out.at[event],
            stat_in.at[event, step - 1],
            stat_send.at[0],
            stat_recv.at[event],
            "tp",
            lax.rem(me + step, count),
        )

    def pack_rows(event, base, ref, first=0, last=groups):
        for group in range(first, last):
            turned = ref[group * LANES : (group + 1) * LANES, :].T
            stat_out[event, base + group : base + group + 1, :] = jnp.sum(
                turned, axis=0, keepdims=True
            )

    def send_stats(event):
        for step in range(1, count):
            stat_copy(event, step).start()

    def total_stats(event):
        total = stat_out[event]
        await_bytes(stat_in.at[event], stat_recv.at[event])
        for step in range(1, count):
            total = total + stat_in[event, step - 1]
        return total

    def spread_rows(ref, packed, base, first=0, last=groups):
        for group in range(first, last):
            line = packed[base + group : base + group + 1, :]
            ref[group * LANES : (group + 1) * LANES, :] = jnp.broadcast_to(
                line, (LANES, LANES)
            ).T

    def strip(index):
        return slice(index * LANES, (index + 1) * LANES)

    def emit_u(layer, half, source):
        def body(start, tile):
            at_rows = pl.ds(start, tile)
            values = source(at_rows)
            squares = jnp.zeros((tile, LANES), jnp.float32)
            for s in range(strips):
                own = values[:, strip(s)]
                squares = squares + own * own
            row_a[at_rows, :] = squares
            gain = pre_ref[layer : layer + 1, pl.ds(pl.multiple_of(me * width, width), width)]
            u_all[layer, me, at_rows, :] = (values * gain).astype(jnp.bfloat16)

        tiles(2 * layer, half, body)

    column_tile = min(256, width)

    def columns(index):
        return pl.ds(pl.multiple_of(index * column_tile, column_tile), column_tile)

    def weigh(projection, block, index):
        at_block = pl.ds(pl.multiple_of(block * width, width), width)
        return w_all[projection, at_block, columns(index)]

    def project_part(which, half, source, keep):
        at_rows = rows_of(0, half)

        def body(index):
            total = None
            for member in range(group):
                for inner in range(blocks_held):
                    block = (2 * member + low_bit) * blocks_held + inner
                    product = jnp.dot(
                        source[block, at_rows, :],
                        weigh(which, block, index),
                        preferred_element_type=jnp.float32,
                    )
                    total = product if total is None else total + product
            keep(at_rows, columns(index), total)

        loop(width // column_tile, body)

    def project_other(which, half):
        def keep(at_rows, at_columns, total):
            half_out[which, at_rows, at_columns] = total.astype(jnp.bfloat16)

        project_part(which, half, x_all, keep)
        half_copy(which, half).start()

    def project_mine(which, half):
        def keep(at_rows, at_columns, total):
            acc[which, at_rows, at_columns] = total

        project_part(which, half, u_all.at[0], keep)

    def project_chip(layer, which, chip, half, first):
        at_rows = rows_of(2 * layer, half)

        def body(index):
            total = None
            for c in range(2):
                product = jnp.dot(
                    u_all[layer, 2 * chip + c, at_rows, :],
                    weigh(3 * layer + which, 2 * chip + c, index),
                    preferred_element_type=jnp.float32,
                )
                total = product if total is None else total + product
            if first:
                acc[which, at_rows, columns(index)] = total
            else:
                acc[which, at_rows, columns(index)] += total

        loop(width // column_tile, body)

    def project_chunk(layer, which, chunk, at_rows):
        offset = (chunk % pieces) * piece

        def body(index):
            total = None
            for owner in range(ring):
                first = owner * depth + offset
                product = jnp.dot(
                    u_all[layer, first // width, at_rows, first % width : first % width + piece],
                    w_all[3 * layer + which, first : first + piece, columns(index)],
                    preferred_element_type=jnp.float32,
                )
                total = product if total is None else total + product
            if chunk % pieces == 0:
                acc[which, at_rows, columns(index)] = total
            else:
                acc[which, at_rows, columns(index)] += total

        loop(width // column_tile, body)

    def gated(layer, half):
        def body(start, tile):
            at_rows = pl.ds(start, tile)
            scale = scale_ref[at_rows, :]
            for s in range(strips):
                value = acc[0, at_rows, strip(s)]
                gate = acc[1, at_rows, strip(s)]
                if layer == 0:
                    value = value + half_in[0, at_rows, strip(s)].astype(jnp.float32)
                    gate = gate + half_in[1, at_rows, strip(s)].astype(jnp.float32)
                value = value * scale
                gate = gate * scale
                glu = (value * (0.5 * (1.0 + jnp.tanh(0.5 * gate)))).astype(jnp.bfloat16)
                padded[s, pl.ds(pl.multiple_of(HALO_ROWS + start, 8), tile), :] = glu.astype(
                    jnp.float32
                )

        tiles(2 * layer, half, body)

    def filter_rows(layer, half):
        def body(start, tile):
            at_rows = pl.ds(start, tile)
            oldest = start + HALO_ROWS - (tap_count - 1)
            first = jnp.zeros((tile, LANES), jnp.float32)
            second = jnp.zeros((tile, LANES), jnp.float32)
            for s in range(strips):
                total = jnp.zeros((tile, LANES), jnp.float32) + bias_ref[
                    layer : layer + 1, strip(s)
                ]
                for tap in range(tap_count):
                    total = (
                        total
                        + padded[s, pl.ds(oldest + tap, tile), :]
                        * tap_rows[layer, tap : tap + 1, strip(s)]
                    )
                f_all[layer, me, at_rows, strip(s)] = total.astype(jnp.bfloat16)
                first = first + total
                second = second + total * total
            row_a[at_rows, :] = first
            row_b[at_rows, :] = second

        tiles(2 * layer + 1, half, body)

    def mix(layer, chip, half):
        for c in range(2):
            block = 2 * chip + c
            gains = params[block, 2 * layer : 2 * layer + 1, :]
            biases = params[block, 2 * layer + 1 : 2 * layer + 2, :]

            def body(start, tile):
                at_rows = pl.ds(start, tile)
                scale = scale_ref[at_rows, :]
                shift = shift_ref[at_rows, :]
                for s in range(strips):
                    shaped = f_all[layer, block, at_rows, strip(s)].astype(jnp.float32) * scale
                    shaped = (shaped - shift) * gains[:, strip(s)] + biases[:, strip(s)]
                    mixed[block, at_rows, strip(s)] = (
                        shaped * (0.5 * (1.0 + jnp.tanh(0.5 * shaped)))
                    ).astype(jnp.bfloat16)

            tiles(2 * layer + 1, half, body)

    def merge(layer, chip, half, first):
        at_rows = rows_of(2 * layer + 1, half)

        def body(index):
            total = None
            for c in range(2):
                block = 2 * chip + c
                product = jnp.dot(
                    mixed[block, at_rows, :],
                    weigh(3 * layer + 2, block, index),
                    preferred_element_type=jnp.float32,
                )
                total = product if total is None else total + product
            if first:
                acc[0, at_rows, columns(index)] = total
            else:
                acc[0, at_rows, columns(index)] += total

        loop(width // column_tile, body)

    for load in loads[:4]:
        load.wait()

    def from_tokens(at_rows):
        return tok_ref[at_rows, :].astype(jnp.float32)

    for half in half_order:
        emit_u(0, half, from_tokens)
    for layer in range(layers):
        params[me, 2 * layer : 2 * layer + 1, :] = ngain_ref[layer : layer + 1, :]
        params[me, 2 * layer + 1 : 2 * layer + 2, :] = nbias_ref[layer : layer + 1, :]
    pack_rows(0, 0, row_a)
    pl.semaphore_wait(
        barrier,
        count + (3 if group > 2 else 1) + has_next.astype(jnp.int32) + has_prev.astype(jnp.int32)
    )

    for chunk in range(2 * pieces):
        for way in range(2):
            sub_copy(chunk, 0, way).start()
    for half in half_order:
        send_own(0, half)

    def param_copy(step):
        return remote(
            params.at[me],
            params.at[me],
            par_send.at[0],
            par_recv.at[0],
            "tp",
            lax.rem(me + step, count),
        )

    for chunk in range(2 * pieces, 3 * pieces):
        ring_copy(chunk, 0, 1 - x_way).start()
    for projection in range(3 * layers):
        own_copy(projection).start()
    send_stats(0)
    for step in range(1, count):
        param_copy(step).start()

    def halo_copy(layer):
        return remote(
            halo_out.at[layer],
            halo_in.at[layer],
            halo_send.at[layer],
            halo_recv.at[layer],
            "sp",
            lax.rem(spot + 1, ring),
        )

    relays = [(index, half) for index in range(chips - 1) for half in half_order]

    def interleave(q, turns_at, chunks, most, after):
        chunks = list(chunks)
        for number, (index, half) in enumerate(relays):
            for _ in range(turns_at.count(number)):
                if chunks:
                    turn_chunk(chunks.pop(0), most)
            relay(q, index, half)
            after(index, half)
        for chunk in chunks:
            turn_chunk(chunk, most)

    def row_scale(event):
        norm = lax.rsqrt(total_stats(event) / model + 1e-06)
        spread_rows(scale_ref, norm, 0)

    def glu_and_halo(layer, half):
        gated(layer, half)
        if half == half_order[0]:
            for s in range(strips):
                halo_out[layer, :, strip(s)] = padded[s, rows : rows + HALO_ROWS, :].astype(
                    jnp.bfloat16
                )

            @pl.when(has_next)
            def _():
                halo_copy(layer).start()

    def emit_f(layer, half):
        if half == 0:

            @pl.when(has_prev)
            def _():
                halo_copy(layer).wait_recv()
                for s in range(strips):
                    padded[s, 0:HALO_ROWS, :] = halo_in[layer, :, strip(s)].astype(jnp.float32)

            @pl.when(spot == 0)
            def _():
                padded[:, 0:HALO_ROWS, :] = jnp.zeros((strips, HALO_ROWS, LANES), jnp.float32)

        filter_rows(layer, half)
        if half == 0:
            event = 4 * layer + 1
            pack_rows(event, 0, row_a)
            pack_rows(event, groups, row_b)
            send_stats(event)
        send_own(2 * layer + 1, half)

    first_out = 2 * pieces
    midway = 5 * pieces + 1
    turns_of = (
        range(second - 1, second + pieces - 1),
        range(second + pieces - 1, 5 * pieces),
        range(5 * pieces, 6 * pieces),
    )

    def first_projections():
        crossings = [(z, half) for half in half_order]
        crossings += [(arrival(index), half) for index, half in relays]
        paced = list(range(first_out, second))
        kept = paced[3:]
        paced = paced[:3]

        def pace():
            if paced:
                ring_copy(paced.pop(0), 0, x_way).start()

        pace()
        pace()

        def after(index, half):
            pace()
            if (index, half) != relays[0]:
                cross(*crossings.pop(0))

        interleave(0, (), (), 0, after)
        for half in half_order:
            side_wait(0, z, half)
            for index in range(chips - 1):
                side_wait(0, arrival(index), half)
        row_scale(0)
        for load in loads[4:]:
            load.wait()
        for each in range(layers):
            for tap in range(tap_count):
                tap_rows[each, tap : tap + 1, :] = taps_ref[tap, each : each + 1, :]
        for which in range(2):
            for chunk in range(which * pieces, (which + 1) * pieces):
                finish_sub(chunk)
            for half in half_order:
                if which == 0:
                    while crossings and crossings[0][1] == half or len(crossings) > 1:
                        cross(*crossings.pop(0))
                    for index in range(-1, chips - 1):
                        cross_wait(z if index < 0 else arrival(index), half)
                project_other(which, half)
            for half in half_order:
                project_mine(which, half)
        for chunk in range(first_out, first_out + pieces // 2):
            turn_chunk(chunk, 0)
        turned = list(range(first_out + pieces // 2, second - 1))
        for half in half_order:
            for which in range(2):
                half_copy(which, half).wait_recv()
            glu_and_halo(0, half)
            if half == half_order[0]:
                for chunk in paced + kept:
                    ring_copy(chunk, 0, x_way).start()
            emit_f(0, half)
            if half == half_order[0]:
                for chunk in turned:
                    turn_chunk(chunk, midway - 1)
    def later_projections(layer):
        base = 3 * layer * pieces

        def chip_of(index):
            return z if index < 0 else arrival(index)

        def take(which, index, half):
            project_chip(layer, which, chip_of(index), half, index < 0)

        def after(index, half):
            if half == half_order[-1] and 0 < index < chips - 2:
                if index == 1:
                    for chunk in range(base, base + pieces):
                        finish_chunk(chunk)
                for done in [-1, 0, 1] if index == 1 else [index]:
                    for each in half_order:
                        side_wait(2 * layer, chip_of(done), each)
                        take(0, done, each)
        interleave(2 * layer, LATE_TURNS, turns_of[1], midway - 1, after)
        for half in half_order:
            side_wait(2 * layer, chip_of(chips - 2), half)
            take(0, chips - 2, half)
        row_scale(4 * layer)
        for chunk in range(base + pieces, base + 2 * pieces - 1):
            finish_chunk(chunk)
            project_chunk(layer, 1, chunk, slice(0, rows))
        finish_chunk(base + 2 * pieces - 1)
        for half in half_order:
            start, size = bounds(2 * layer, half)
            project_chunk(layer, 1, base + 2 * pieces - 1, slice(start, start + size))
            glu_and_halo(layer, half)
            if half == half_order[0]:
                start_until(midway + AHEAD - 1)
            emit_f(layer, half)

    def merge_chunk(layer, chunk, first):
        offset = (chunk % pieces) * piece

        def body(index):
            total = None
            for each in range(-1, chips - 2):
                chip = z if each < 0 else arrival(each)
                for c in range(2):
                    if c % blocks_held != offset // width:
                        continue
                    block = 2 * chip + c
                    start = block * width + offset % width
                    product = jnp.dot(
                        mixed[block, :, offset % width : offset % width + piece],
                        w_all[
                            3 * layer + 2, pl.ds(pl.multiple_of(start, piece), piece), columns(index)
                        ],
                        preferred_element_type=jnp.float32,
                    )
                    total = product if total is None else total + product
            if first:
                acc[0, :, columns(index)] = total
            else:
                acc[0, :, columns(index)] += total

        loop(width // column_tile, body)

    def squares(layer, start, tile):
        at_rows = pl.ds(start, tile)
        total = jnp.zeros((tile, LANES), jnp.float32)
        for s in range(strips):
            branch = acc[0, at_rows, strip(s)].astype(jnp.bfloat16)
            if layer == layers - 1:
                last[at_rows, strip(s)] = branch
            own = branch.astype(jnp.float32)
            total = total + own * own
        row_b[at_rows, :] = total

    def settle():
        sent = 2 * ((group_turns - 1) * piece + piece // 2)
        await_bytes(w_all.at[0, 0 : 2 * pieces * sent, :], sub_send.at[0])
        for chunk in range(chunk_total - 2 * pieces):
            await_bytes(
                w_all.at[0, 0 : 2 * ((turns - 1) * piece + piece // 2), :], ring_send.at[chunk]
            )
        for which in range(2):
            for half in range(HALVES):
                half_copy(which, half).wait_send()
        for q in range(2 * layers):
            drain(q)
        await_bytes(stat_in, stat_send.at[0])
        await_bytes(params.at[0 : count - 1], par_send.at[0])

        @pl.when(has_next)
        def _():
            for layer in range(layers):
                halo_copy(layer).wait_send()

    for layer in range(layers):
        q = 2 * layer
        event = 4 * layer
        base = 3 * layer * pieces
        if layer == 0:
            first_projections()
        else:
            later_projections(layer)

        def normal(layer=layer, event=event):
            totals = total_stats(event + 1) / model
            centre = totals[0:groups, :]
            spread = jnp.maximum(totals[groups : 2 * groups, :] - centre * centre, 0.0)
            inverse = lax.rsqrt(spread + 1e-05)
            spread_rows(scale_ref, inverse, 0)
            spread_rows(shift_ref, centre * inverse, 0)
            if layer == 0:
                await_bytes(params.at[0 : count - 1], par_recv.at[0])
            for half in half_order:
                side_wait(2 * layer + 1, z, half)
                mix(layer, z, half)

        def ready(index, half, layer=layer, normal=normal):
            q = 2 * layer + 1
            if index == 0 and half == half_order[0]:
                return
            if index == 0:
                normal()
                for again in half_order:
                    side_wait(q, arrival(0), again)
                    mix(layer, arrival(0), again)
                return
            if index == chips - 2 and half == half_order[0]:
                for chunk in range((3 * layer + 2) * pieces, (3 * layer + 3) * pieces):
                    finish_chunk(chunk)
                    merge_chunk(layer, chunk, chunk % pieces == 0)
            side_wait(q, arrival(index), half)
            mix(layer, arrival(index), half)
            if index == chips - 2:
                merge(layer, arrival(index), half, False)
                tiles(q, half, functools.partial(squares, layer))
                pack_rows(4 * layer + 3 - half, 0, row_b, *groups_of(q, half))
                send_stats(4 * layer + 3 - half)

        interleave(
            q + 1,
            LAST_TURNS if layer else OUT_TURNS,
            turns_of[2] if layer else turns_of[0],
            chunk_total if layer else midway - 1,
            ready,
        )
        def updated(at_rows, layer=layer):
            branch = acc[0, at_rows, :].astype(jnp.bfloat16).astype(jnp.float32)
            scale = jnp.concatenate([scale_ref[at_rows, :]] * strips, axis=1)
            before = (tok_ref if layer == 0 else stream)[at_rows, :].astype(jnp.float32)
            after = before + branch * scale * post_ref[layer : layer + 1, :]
            after = after.astype(jnp.bfloat16)
            stream[at_rows, :] = after
            return after.astype(jnp.float32)

        if layer == layers - 1:
            settle()
        for half in half_order:
            totals = total_stats(event + 3 - half)
            if layer + 1 < layers:
                scale = lax.rsqrt(totals / model + 1e-06)
                spread_rows(scale_ref, scale, 0, *groups_of(q + 1, half))
                emit_u(layer + 1, half, updated)
                send_own(q + 2, half)
                if half == 0:
                    pack_rows(event + 4, 0, row_a)
                    send_stats(event + 4)
            else:
                first, end = groups_of(q + 1, half)
                final[first:end, :] = totals[first:end, :]

    gain_ref[...] = post_ref[layers - 1 : layers, :]
    if layers == 1:
        stream[...] = tok_ref[...]


def shards(
    tokens, pre_gain, w_value, w_gate, conv_taps, conv_bias, norm_gain, norm_bias, w_out, post_gain
):
    ring = lax.axis_size("sp")
    count = lax.axis_size("tp")
    chips = count // 2
    layers, depth, width = w_value.shape
    rows = tokens.shape[0]
    pieces = max(1, min(4, depth // 256))
    chunks = 3 * layers * pieces
    strips = width // LANES
    stat_rows = max(8, 2 * rows // LANES)
    param_rows = -(-2 * layers // 8) * 8
    hbm = pl.BlockSpec(memory_space=pl.ANY)
    dma = pltpu.SemaphoreType.DMA
    taps = jnp.transpose(conv_taps, (1, 0, 2))
    loaded = [tokens, pre_gain, taps, conv_bias, norm_gain, norm_bias, post_gain]
    scratch = [pltpu.VMEM(array.shape, array.dtype) for array in loaded]
    scratch += [dma((len(loaded),))]
    scratch += [pltpu.VMEM(conv_taps.shape, conv_taps.dtype)]
    scratch += [
        pltpu.VMEM((3 * layers, depth * ring, width), jnp.bfloat16),
        pltpu.VMEM((layers, count, rows, width), jnp.bfloat16),
        pltpu.VMEM((layers, count, rows, width), jnp.bfloat16),
        pltpu.VMEM((count, rows, width), jnp.bfloat16),
        pltpu.VMEM((2, rows, width), jnp.float32),
        pltpu.VMEM((strips, HALO_ROWS + rows, LANES), jnp.float32),
        pltpu.VMEM((rows, LANES), jnp.float32),
        pltpu.VMEM((rows, LANES), jnp.float32),
        pltpu.VMEM((rows, LANES), jnp.float32),
        pltpu.VMEM((rows, LANES), jnp.float32),
        pltpu.VMEM((layers, HALO_ROWS, width), jnp.bfloat16),
        pltpu.VMEM((layers, HALO_ROWS, width), jnp.bfloat16),
        pltpu.VMEM((4 * layers, stat_rows, LANES), jnp.float32),
        pltpu.VMEM((4 * layers, count - 1, stat_rows, LANES), jnp.float32),
        pltpu.VMEM((count, param_rows, width), jnp.float32),
        pltpu.VMEM((count, rows, width), jnp.bfloat16),
        pltpu.VMEM((2, rows, width), jnp.bfloat16),
        pltpu.VMEM((2, rows, width), jnp.bfloat16),
    ]
    scratch += [dma((2 * layers,))] * 2 + [dma((2 * layers, chips, HALVES))]
    scratch += [dma((2 * layers,)), dma((2 * layers, chips, HALVES))]
    scratch += [dma((chunks - 2 * pieces,)), dma((chunks - 2 * pieces, ring // 2))]
    scratch += [dma((1,)), dma((2, 2 * pieces, max(1, ring // 4)))]
    scratch += [dma((3 * layers,))]
    scratch += [dma((chips, HALVES))] * 4
    scratch += [dma((2, HALVES))] * 2
    scratch += [dma((1,)), dma((4 * layers,))]
    scratch += [dma((1,)), dma((1,))]
    scratch += [dma((layers,))] * 2
    flops = 2 * rows * model_width(tokens, count) * width * 3 * layers
    branch, before, totals, gain = pl.pallas_call(
        functools.partial(module_kernel, ring, count),
        out_shape=[
            pltpu.VMEM(tokens.shape, tokens.dtype),
            pltpu.VMEM(tokens.shape, tokens.dtype),
            pltpu.VMEM((stat_rows, LANES), jnp.float32),
            pltpu.VMEM((1, width), jnp.float32),
        ],
        in_specs=[hbm] * 10,
        out_specs=[pl.BlockSpec(memory_space=pltpu.VMEM)] * 4,
        scratch_shapes=scratch,
        compiler_params=pltpu.CompilerParams(
            collective_id=0, has_side_effects=True, vmem_limit_bytes=60 * 2**20
        ),
        cost_estimate=pl.CostEstimate(flops=flops, bytes_accessed=flops // 512, transcendentals=0),
        name="modules",
    )(
        tokens,
        pre_gain,
        w_value,
        w_gate,
        w_out,
        taps,
        conv_bias,
        norm_gain,
        norm_bias,
        post_gain,
    )
    total = totals[: rows // LANES].reshape(rows)
    rescale = lax.rsqrt(total / model_width(tokens, count) + 1e-06)[:, None]
    after = before.astype(jnp.float32) + branch.astype(jnp.float32) * rescale * gain
    return after.astype(jnp.bfloat16)


def model_width(tokens, count):
    return tokens.shape[1] * count


def solution(mesh):
    in_specs = (
        P("sp", "tp"),
        P(),
        P(None, "sp", "tp"),
        P(None, "sp", "tp"),
        P(None, None, "tp"),
        P(None, "tp"),
        P(None, "tp"),
        P(None, "tp"),
        P(None, "sp", "tp"),
        P(None, "tp"),
    )
    out_specs = P("sp", "tp")
    return jax.shard_map(shards, mesh=mesh, in_specs=in_specs, out_specs=out_specs, check_vma=False)
```
